512 devices in a mesh: sp: 64 (over z, y), tp: 8 (over x, core).
Axes of the slice: x: 4, y: 8, z: 8, core: 2. Of those that a mesh axis runs over, the one named last changes fastest.
Arguments:
- residual_in: bfloat16 [16384, 2048], P(('sp', 'tp')), may hold values from -6 to 6
- query_lean: bfloat16 [16384, 8, 96], P('sp', 'tp'), may hold values from -60 to 60
- query_broad: bfloat16 [16384, 8, 160], P('sp', 'tp'), may hold values from -60 to 60
- latent: bfloat16 [16384, 256], P('sp'), may hold values from -6 to 6
- rope_key: bfloat16 [16384, 32], P('sp'), may hold values from -8 to 8
- latent_gain: float32 [256], replicated, may hold values from 0.1 to 1.9
- key_up_lean: bfloat16 [256, 8, 64], P(None, 'tp'), may hold values from -0.375 to 0.375
- key_up_broad: bfloat16 [256, 8, 128], P(None, 'tp'), may hold values from -0.375 to 0.375
- value_up_lean: bfloat16 [256, 8, 64], P(None, 'tp'), may hold values from -0.375 to 0.375
- value_up_broad: bfloat16 [256, 8, 128], P(None, 'tp'), may hold values from -0.375 to 0.375
- out_lean: bfloat16 [8, 64, 2048], P('tp'), may hold values from -0.15625 to 0.15625
- out_broad: bfloat16 [8, 128, 2048], P('tp'), may hold values from -0.15625 to 0.15625
- attn_gain: float32 [2048], replicated, may hold values from 0.1 to 1.9
- mlp_gain: float32 [2048], replicated, may hold values from 0.1 to 1.9
- gate_weight: bfloat16 [2048, 2816], P('sp', 'tp'), may hold values from -0.125 to 0.125
- up_weight: bfloat16 [2048, 2816], P('sp', 'tp'), may hold values from -0.125 to 0.125
- down_weight: bfloat16 [2816, 2048], P('tp', 'sp'), may hold values from -0.109375 to 0.109375
Outputs:
- layer_out: bfloat16 [16384, 2048], P(('sp', 'tp'))
The draws below stay inside these ranges and needn't reach their ends.
All inputs are finite; a program needn't handle non-finite values.
Results may differ from the reference program's by a relative error of at most 0.015.
Values may be sent and summed in bfloat16 or wider, within the bound.
A program may use at most 128 MiB of HBM per device.

```python
import math
import jax
import jax.numpy as jnp
from jax import lax

D = 2048
HEADS_A = 8
HEADS_B = 8
NOPE_A = 64
V_A = 64
NOPE_B = 128
V_B = 128
ROPE = 32
KV_RANK = 256
FF = 2816
QK_A = 96
QK_B = 160
TOKENS = 16384
N_TP = 8


def draw_rope_key(key, part):
    base = jax.random.truncated_normal(jax.random.fold_in(key, 1), -4.0, 4.0, (TOKENS, ROPE), jnp.float32)
    return base.astype(jnp.bfloat16)


def draw_query_lean(key, part):
    base = jax.random.truncated_normal(jax.random.fold_in(key, 2), -4.0, 4.0, (TOKENS, HEADS_A, QK_A), jnp.float32)
    return base.astype(jnp.bfloat16)


def draw_query_broad(key, part):
    base = jax.random.truncated_normal(jax.random.fold_in(key, 3), -4.0, 4.0, (TOKENS, HEADS_B, QK_B), jnp.float32)
    return base.astype(jnp.bfloat16)


def levels(key, extent, pieces, smallest, high):
    def one(position, shards_of):
        heights = jax.random.uniform(jax.random.fold_in(jax.random.fold_in(key, 6), position), (shards_of,), jnp.float32, smallest / len(pieces), high / len(pieces))
        return jnp.repeat(jnp.exp(heights), extent[position] // shards_of).reshape((-1,) + (1,) * (len(extent) - position - 1))

    factor_of = one(*pieces[0])
    for cut in pieces[1:]:
        factor_of = factor_of * one(*cut)
    return factor_of


def centred(own_key, extent, scale, bound, cuts=(), held_as=jnp.bfloat16):
    loudness = levels(own_key, extent, cuts, -0.22, 0.18) if cuts else 1.0
    values = jax.random.normal(own_key, extent, jnp.float32) * scale * loudness
    return jnp.minimum(jnp.maximum(values, -bound), bound).astype(held_as)


def setup_inputs(seed: int = 0) -> dict:
    seeds = jax.random.split(jax.random.key(seed), 18)
    return {
        "residual_in": centred(seeds[0], (TOKENS, D), 1.0, 6.0, ((0, 512),)),
        "query_lean": draw_query_lean(jax.random.fold_in(seeds[17], 71), 0),
        "query_broad": draw_query_broad(jax.random.fold_in(seeds[17], 71), 0),
        "latent": centred(seeds[3], (TOKENS, KV_RANK), 1.0, 6.0, ((0, 64),)),
        "rope_key": draw_rope_key(jax.random.fold_in(seeds[17], 71), 0),
        "latent_gain": jnp.clip(1.0 + 0.18 * jax.random.normal(seeds[5], (KV_RANK,), jnp.float32), 0.1, 1.9),
        "key_up_lean": centred(seeds[6], (KV_RANK, HEADS_A, NOPE_A), KV_RANK ** -0.5, 0.375, ((1, 8),)),
        "key_up_broad": centred(seeds[7], (KV_RANK, HEADS_B, NOPE_B), KV_RANK ** -0.5, 0.375, ((1, 8),)),
        "value_up_lean": centred(seeds[8], (KV_RANK, HEADS_A, V_A), KV_RANK ** -0.5, 0.375, ((1, 8),)),
        "value_up_broad": centred(seeds[9], (KV_RANK, HEADS_B, V_B), KV_RANK ** -0.5, 0.375, ((1, 8),)),
        "out_lean": centred(seeds[10], (HEADS_A, V_A, D), (HEADS_A * V_A + HEADS_B * V_B) ** -0.5, 0.15625, ((0, 8),)),
        "out_broad": centred(seeds[11], (HEADS_B, V_B, D), (HEADS_A * V_A + HEADS_B * V_B) ** -0.5, 0.15625, ((0, 8),)),
        "attn_gain": jnp.clip(1.0 + 0.18 * jax.random.normal(seeds[12], (D,), jnp.float32), 0.1, 1.9),
        "mlp_gain": jnp.clip(1.0 + 0.18 * jax.random.normal(seeds[13], (D,), jnp.float32), 0.1, 1.9),
        "gate_weight": centred(seeds[14], (D, FF), D ** -0.5, 0.125, ((0, 64), (1, 8))),
        "up_weight": centred(seeds[15], (D, FF), D ** -0.5, 0.125, ((0, 64), (1, 8))),
        "down_weight": centred(seeds[16], (FF, D), FF ** -0.5, 0.109375, ((0, 8), (1, 64))),
    }


THETA = 10000.0
EPS = 1e-06
NEGATIVE = -1e+30

def rotate(values, positions):
    width = values.shape[-1]
    half = width // 2
    freqs = THETA ** (-2.0 * jnp.arange(half, dtype=jnp.float32) / width)
    angle = positions.astype(jnp.float32)[:, None] * freqs[None, :]
    cosine = jnp.cos(angle)
    sine = jnp.sin(angle)
    if values.ndim == 3:
        cosine = cosine[:, None, :]
        sine = sine[:, None, :]
    first = values[..., :half]
    second = values[..., half:]
    return jnp.concatenate([first * cosine - second * sine, first * sine + second * cosine], axis=-1)

def normalize(values, gain):
    return values * lax.rsqrt(lax.optimization_barrier(jnp.mean(values * values, axis=-1, keepdims=True)) + EPS) * gain.astype(jnp.float32)

def widen(values):
    return lax.optimization_barrier(values).astype(jnp.float32)

def attend_group(query, key_up, value_up, latent_normed, rotated_key, positions):
    nope = key_up.shape[2]
    heads = key_up.shape[1]
    vsize = value_up.shape[2]
    scale = query.shape[2] ** (-0.5)
    lat = latent_normed.astype(jnp.float32)
    keys = widen(jnp.einsum('kr,rhd->khd', lat, key_up.astype(jnp.float32)).astype(jnp.bfloat16))
    values = widen(jnp.einsum('kr,rhd->khd', lat, value_up.astype(jnp.float32)).astype(jnp.bfloat16))
    rot_keys = rotated_key.astype(jnp.float32)
    query_nope = query[:, :, :nope].astype(jnp.float32)
    query_rot = widen(rotate(query[:, :, nope:].astype(jnp.float32), positions).astype(jnp.bfloat16))
    size = math.gcd(TOKENS, 256)

    def block(index):
        start = (index * size).astype(jnp.int32)
        rows = start + jnp.arange(size, dtype=jnp.int32)
        part_nope = lax.dynamic_slice_in_dim(query_nope, start, size, 0)
        part_rot = lax.dynamic_slice_in_dim(query_rot, start, size, 0)
        scores = (jnp.einsum('qhd,khd->hqk', part_nope, keys) + jnp.einsum('qhr,kr->hqk', part_rot, rot_keys)) * scale
        visible = positions[None, :] <= rows[:, None]
        scores = jnp.where(visible[None], scores, NEGATIVE)
        peak = lax.optimization_barrier(jnp.max(scores, axis=-1, keepdims=True))
        weights = jnp.where(visible[None], jnp.exp(scores - peak), 0.0)
        total = lax.optimization_barrier(jnp.sum(weights, axis=-1))
        rounded = widen(weights.astype(jnp.bfloat16))
        result = jnp.einsum('hqk,khv->qhv', rounded, values) / jnp.transpose(total)[:, :, None]
        return result.astype(jnp.bfloat16)
    blocks = lax.map(block, jnp.arange(TOKENS // size, dtype=jnp.int32))
    return blocks.reshape(TOKENS, heads, vsize)

def reference(residual_in, query_lean, query_broad, latent, rope_key, latent_gain, key_up_lean, key_up_broad, value_up_lean, value_up_broad, out_lean, out_broad, attn_gain, mlp_gain, gate_weight, up_weight, down_weight):
    positions = jnp.arange(TOKENS, dtype=jnp.int32)
    latent_normed = normalize(latent.astype(jnp.float32), latent_gain).astype(jnp.bfloat16)
    rotated_key = rotate(rope_key.astype(jnp.float32), positions).astype(jnp.bfloat16)
    attended_lean = attend_group(query_lean, key_up_lean, value_up_lean, latent_normed, rotated_key, positions)
    attended_broad = attend_group(query_broad, key_up_broad, value_up_broad, latent_normed, rotated_key, positions)
    lean_per = HEADS_A // N_TP
    broad_per = HEADS_B // N_TP
    head_sum = jnp.zeros((TOKENS, D), jnp.float32)
    for group in range(N_TP):
        partial_value = jnp.einsum('qhv,hvd->qd', attended_lean[:, group * lean_per:(group + 1) * lean_per].astype(jnp.float32), out_lean[group * lean_per:(group + 1) * lean_per].astype(jnp.float32))
        partial_value = partial_value + jnp.einsum('qhv,hvd->qd', attended_broad[:, group * broad_per:(group + 1) * broad_per].astype(jnp.float32), out_broad[group * broad_per:(group + 1) * broad_per].astype(jnp.float32))
        head_sum = head_sum + partial_value.astype(jnp.bfloat16).astype(jnp.float32)
    branch = normalize(head_sum, attn_gain)
    mixed = (residual_in.astype(jnp.float32) + branch).astype(jnp.bfloat16)
    normed = normalize(mixed.astype(jnp.float32), mlp_gain).astype(jnp.bfloat16)
    gate = jnp.dot(normed, gate_weight, preferred_element_type=jnp.float32)
    up = jnp.dot(normed, up_weight, preferred_element_type=jnp.float32)
    hidden = (jax.nn.silu(gate) * up).astype(jnp.bfloat16)
    units = FF // N_TP
    channel_sum = jnp.zeros((TOKENS, D), jnp.float32)
    for group in range(N_TP):
        partial_value = jnp.dot(hidden[:, group * units:(group + 1) * units], down_weight[group * units:(group + 1) * units], preferred_element_type=jnp.float32)
        channel_sum = channel_sum + partial_value.astype(jnp.bfloat16).astype(jnp.float32)
    return (mixed.astype(jnp.float32) + 0.5 * channel_sum).astype(jnp.bfloat16)
```

```python
import functools

import jax
import jax.numpy as jnp
from jax import lax
from jax.experimental import pallas as pl
from jax.experimental.pallas import tpu as pltpu
from jax.sharding import PartitionSpec as P

MESH = pl.DeviceIdType.MESH
THETA = 10000.0
EPS = 1e-06
NEGATIVE = -1e30
LOG2E = 1.4426950408889634
RING = 8
LAG = 3
F32 = jnp.float32
BF16 = jnp.bfloat16

HALF = 128
PIECE = HALF + 16


def rem(v, n):
    return lax.rem(v, jnp.int32(n))


def div(v, n):
    return lax.div(v, jnp.int32(n))


def kernel(
    pieces, queries, kb, kl, vb, vl, ob, ol, resid, again, mgain, gate_w, up_w, down_w,
    out,
    lat, wts, wout, rows, att, qt, kup, vupt, spread, peak, total, accum, att_t, hs, norm, hid, part, pbuf, sbuf, rbuf, wown,
    l_recv, l_first, l_plus, l_minus, p_recv, p_send,
    w_recv, w_first, w_plus, w_minus,
    loc, o_send, o_recv, r_send, r_recv, a_send, a_recv, s_send, s_recv,
):
    sp = lax.axis_index("sp")
    tp = lax.axis_index("tp")
    core = rem(tp, 2)
    xx = div(tp, 2)
    other = 1 - core
    sa = 1 + 7 * core
    sb = 8 - 7 * core
    a = rem(lax.div(sp, sa), RING)
    b = rem(lax.div(sp, sb), RING)

    def at(first, second):
        return rem(first + 16, RING) * sa + rem(second + 16, RING) * sb

    def turned(first, second):
        return rem(first + 16, RING) * sb + rem(second + 16, RING) * sa

    def rel(k):
        return div(k + 1, 2) * (1 - 2 * rem(k, 2))

    a_up, a_dn, b_up, b_dn = (
        (at(a + 1, b), tp), (at(a - 1, b), tp), (at(a, b + 1), tp), (at(a, b - 1), tp)
    )
    partner = (sp, 2 * xx + other)

    def across(step):
        return 2 * rem(xx + step, 4) + core

    x_up, x_far, x_dn = (sp, across(1)), (sp, across(2)), (sp, across(3))

    def remote(src, dst, ssem, rsem, dev):
        return pltpu.make_async_remote_copy(
            src_ref=src, dst_ref=dst, send_sem=ssem, recv_sem=rsem, device_id=dev, device_id_type=MESH
        )

    own_b = pltpu.make_async_copy(ob, wout.at[tp, pl.ds(0, 128)], loc.at[0])
    own_l = pltpu.make_async_copy(ol, wout.at[tp, pl.ds(128, 64)], loc.at[1])
    own_r = pltpu.make_async_copy(resid, rows.at[tp], loc.at[2])
    own_b.start()
    own_l.start()
    own_r.start()

    barrier = pltpu.get_barrier_semaphore()
    for dev in (a_up, a_dn, b_up, b_dn, partner, x_up, x_far, x_dn):
        pl.semaphore_signal(barrier, inc=1, device_id=dev, device_id_type=MESH)
    pl.semaphore_wait(barrier, 8)

    class Stream:
        def __init__(self, own, slot, recv, first, plus, minus, push):
            self.own, self.slot, self.recv = own, slot, recv
            self.first, self.plus, self.minus, self.push = first, plus, minus, push

        def send(self, src, o, ssem, dev):
            return remote(src, self.slot(o), ssem, self.recv.at[o], dev)

        def start(self):
            for index, dev in ((0, a_up), (7, a_dn)):
                self.send(self.own, sp, self.first.at[index], dev).start()
            self.send(self.own, sp, self.plus.at[0], b_up).start()
            self.send(self.own, sp, self.minus.at[0], b_dn).start()

        def arrived(self, o):
            self.send(self.slot(o), o, self.first.at[0], partner).wait_recv()

        def near(self, k):
            o = at(a + rel(k), b)
            self.arrived(o)

            @pl.when((rem(k, 2) == 1) & (k < 7))
            def _():
                self.send(self.slot(o), o, self.first.at[k], a_up).start()

            @pl.when((rem(k, 2) == 0) & (k < 6))
            def _():
                self.send(self.slot(o), o, self.first.at[k], a_dn).start()

            self.send(self.slot(o), o, self.plus.at[k], b_up).start()
            self.send(self.slot(o), o, self.minus.at[k], b_dn).start()
            if self.push:
                self.give(o)

        def give(self, o):
            remote(self.slot(o), self.slot(o), p_send.at[o], p_recv.at[o], partner).start()

        def far(self, n):
            kp, km, d = ring_step(n)
            op, om = at(a + rel(kp), b - d), at(a + rel(km), b + d)
            self.arrived(op)

            @pl.when(n < 28)
            def _():
                self.send(self.slot(op), op, self.plus.at[n], b_up).start()

            if self.push:
                self.give(op)
            self.arrived(om)

            @pl.when((n < 24) | ((n >= 28) & (n < 32)))
            def _():
                self.send(self.slot(om), om, self.minus.at[n], b_dn).start()

            if self.push:
                self.give(om)

        def step(self, n):
            @pl.when((n >= 1) & (n < 8))
            def _():
                self.near(n)

            @pl.when((n >= 8) & (n < 36))
            def _():
                self.far(n)

        def drain(self):
            def sent(sem):
                remote(self.slot(sp), self.slot(sp), sem, self.recv.at[sp], partner).wait_send()

            for index in (0, 1, 2, 3, 4, 5, 7):
                sent(self.first.at[index])

            @pl.loop(0, 28)
            def _(n):
                sent(self.plus.at[n])

            @pl.loop(0, 24)
            def _(n):
                sent(self.minus.at[n])

            @pl.loop(28, 32)
            def _(n):
                sent(self.minus.at[n])

    def ring_step(n):
        last = div(n, 32)
        kp = rem(n, 8)
        return kp, kp + 4 * last, div(n, 8)

    latents = Stream(
        pieces.at[core], lambda o: lat.at[core, o], l_recv, l_first, l_plus, l_minus, True
    )
    weights = Stream(wown, lambda o: wts.at[o], w_recv, w_first, w_plus, w_minus, False)
    latents.start()

    own_r.wait()
    for i, dev in enumerate((partner, x_up, x_dn, x_far)):
        remote(rows.at[tp], rows.at[tp], r_send.at[i], r_recv.at[tp], dev).start()
    own_b.wait()
    own_l.wait()
    for i, dev in enumerate((partner, x_up, x_dn)):
        remote(wout.at[tp], wout.at[tp], o_send.at[i], o_recv.at[tp], dev).start()

    def share_rows():
        for i in (1, 2, 3):
            t = across(i)
            remote(rows.at[t], rows.at[t], r_send.at[3 + i], r_recv.at[t], partner).wait_recv()
            remote(rows.at[t], rows.at[t], r_send.at[3 + i], r_recv.at[t], partner).start()

    top, low = pl.ds(0, 96), pl.ds(96, 96)

    def share_near():
        for i, t, rest, dev in ((3, across(3), top, x_up), (4, across(1), low, x_dn)):
            remote(wout.at[t], wout.at[t], o_send.at[i], o_recv.at[t], partner).wait_recv()
            far = 8 if i == 3 else 9
            remote(wout.at[t, rest], wout.at[t, rest], o_send.at[i], o_recv.at[far], dev).start()
            remote(wout.at[t], wout.at[t], o_send.at[i + 2], o_recv.at[t], partner).start()

    def share_far():
        t = across(2)
        for i, rest in ((8, top), (9, low)):
            remote(wout.at[t, rest], wout.at[t, rest], o_send.at[0], o_recv.at[i], partner).wait_recv()
            remote(wout.at[t, rest], wout.at[t, rest], o_send.at[i - 1], o_recv.at[i + 2], partner).start()

    qt[...] = queries[...].T
    kup[...] = jnp.zeros_like(kup)
    kup[:, 0:128] = kb[...]
    kup[:, 128:192] = kl[...]
    vupt[0:128, :] = vb[...].T
    vupt[128:192, :] = vl[...].T
    spread[...] = (
        lax.broadcasted_iota(jnp.int32, (32, 256), 1) == lax.broadcasted_iota(jnp.int32, (32, 256), 0) + 192
    ).astype(F32).astype(BF16)
    wown[...] = jnp.zeros_like(wown)
    wown[:, 0:352] = gate_w[...]
    wown[:, 384:736] = up_w[...]
    wown[:, 768:1120] = down_w[...].T

    column = lax.broadcasted_iota(jnp.int32, (1, 512), 1)
    factor = jnp.where(column < 256, LOG2E * 160 ** (-0.5), LOG2E * 96 ** (-0.5)).astype(F32)

    def project(halves):
        rows_of = jnp.concatenate([h[0:HALF, :] for h in halves], axis=0)
        turned_rot = jnp.concatenate(
            [
                jnp.concatenate([h[HALF:PIECE, 0:HALF] for h in halves], axis=1),
                jnp.concatenate([h[HALF:PIECE, HALF:256] for h in halves], axis=1),
            ],
            axis=0,
        )
        keys = jnp.dot(rows_of, kup[...], preferred_element_type=F32) + lax.dot_general(
            turned_rot, spread[...], (((0,), (0,)), ((), ())), preferred_element_type=F32
        )
        values = lax.dot_general(
            vupt[...], rows_of, (((1,), (1,)), ((), ())), preferred_element_type=F32
        )
        return keys.astype(BF16), values.astype(BF16)

    def fold(halves, blocks):
        keys, values = project(halves)
        scores = jnp.dot(keys, qt[...], preferred_element_type=F32) * factor
        if blocks is None:
            seen = lax.broadcasted_iota(jnp.int32, scores.shape, 0) <= (
                lax.broadcasted_iota(jnp.int32, scores.shape, 1) & 255
            )
            scores = jnp.where(seen, scores, NEGATIVE)
        else:
            scores = jnp.concatenate(
                [
                    scores[i * HALF : (i + 1) * HALF] + jnp.where(o <= sp, 0.0, NEGATIVE).astype(F32)
                    for i, o in enumerate(blocks)
                ],
                axis=0,
            )
        old = peak[...]
        new = jnp.maximum(old, jnp.max(scores, axis=0, keepdims=True))
        shrink = jnp.exp2(old - new)
        wt = jnp.exp2(scores - new)
        peak[...] = new
        total[...] = total[...] * shrink + jnp.sum(wt, axis=0, keepdims=True)
        wt = wt.astype(BF16)
        accum[0:128, :] = accum[0:128, :] * shrink[:, 0:256] + jnp.dot(
            values[0:128], wt[:, 0:256], preferred_element_type=F32
        )
        accum[128:192, :] = accum[128:192, :] * shrink[:, 256:512] + jnp.dot(
            values[128:192], wt[:, 256:512], preferred_element_type=F32
        )

    peak[...] = jnp.full_like(peak, NEGATIVE)
    total[...] = jnp.zeros_like(total)
    accum[...] = jnp.zeros_like(accum)
    fold([pieces.at[0], pieces.at[1]], None)

    def given(o):
        remote(lat.at[other, o], lat.at[other, o], p_send.at[0], p_recv.at[o], partner).wait_recv()

    def compute(n):
        @pl.when((n >= 1) & (n < 8))
        def _():
            o1, o2 = at(a + rel(n), b), turned(b + rel(n), a)
            given(o2)

            @pl.when(jnp.minimum(o1, o2) <= sp)
            def _():
                fold([lat.at[core, o1], lat.at[other, o2]], (o1, o2))

        @pl.when((n >= 8) & (n < 36))
        def _():
            kp, km, d = ring_step(n)
            o1, o2 = at(a + rel(kp), b - d), at(a + rel(km), b + d)
            o3, o4 = turned(b + rel(kp), a - d), turned(b + rel(km), a + d)
            given(o3)
            given(o4)

            @pl.when(jnp.minimum(jnp.minimum(o1, o2), jnp.minimum(o3, o4)) <= sp)
            def _():
                fold(
                    [lat.at[core, o1], lat.at[core, o2], lat.at[other, o3], lat.at[other, o4]],
                    (o1, o2, o3, o4),
                )

    @pl.loop(1, 36 + LAG)
    def _(n):
        latents.step(n)

        @pl.when(n == 36)
        def _():
            weights.start()

        @pl.when(n >= 37)
        def _():
            weights.step(n - 36)

        @pl.when(n == 20)
        def _():
            share_rows()

        @pl.when(n == 28)
        def _():
            share_near()

        compute(n - LAG)

    result = accum[...]
    att[tp, 0:128, :] = (result[0:128] / total[:, 0:256]).astype(BF16)
    att[tp, 128:192, :] = (result[128:192] / total[:, 256:512]).astype(BF16)

    weights.step(jnp.int32(LAG))

    for i, dev in enumerate((x_far, x_up, x_dn, partner)):
        remote(att.at[tp], att.at[tp], a_send.at[i], a_recv.at[tp], dev).start()

    @pl.loop(LAG + 1, 8)
    def _(n):
        weights.step(n)

    share_far()
    for i in (1, 3, 2):
        t = across(i)
        remote(att.at[t], att.at[t], a_send.at[0], a_recv.at[t], partner).wait_recv()
        remote(att.at[t], att.at[t], a_send.at[3 + i], a_recv.at[t], partner).start()

    @pl.loop(8, 10)
    def _(n):
        weights.step(n)

    for i in (0, 1, 2, 3):
        t = 2 * rem(xx + i, 4) + other
        remote(att.at[t], att.at[t], a_send.at[0], a_recv.at[t], partner).wait_recv()
        remote(rows.at[t], rows.at[t], r_send.at[0], r_recv.at[t], partner).wait_recv()
        if i == 2:
            for j, rest in ((10, top), (11, low)):
                remote(wout.at[t, rest], wout.at[t, rest], o_send.at[0], o_recv.at[j], partner).wait_recv()
        else:
            remote(wout.at[t], wout.at[t], o_send.at[0], o_recv.at[t], partner).wait_recv()

    @pl.loop(0, 8)
    def _(t):
        att_t[t] = att[t].T

    @pl.loop(0, 8)
    def _(j):
        cols = pl.ds(pl.multiple_of(j * 256, 256), 256)
        acc = jnp.dot(att_t[0], wout[0, :, cols], preferred_element_type=F32)
        for t in range(1, 8):
            acc = acc + jnp.dot(att_t[t], wout[t, :, cols], preferred_element_type=F32)
        hs[:, cols] = acc
        weights.step(10 + j)

    for i in range(7):
        remote(rows.at[tp], rows.at[tp], r_send.at[i], r_recv.at[tp], partner).wait_send()

    @pl.loop(0, 8)
    def _(t):
        chunk = pl.ds(pl.multiple_of(t * 32, 32), 32)
        value = hs[chunk, :]
        scale = lax.rsqrt(jnp.mean(value * value, axis=-1, keepdims=True) + EPS)
        mixed = (rows[t].astype(F32) + value * scale * again[...]).astype(BF16)
        rows[t] = mixed
        value = mixed.astype(F32)
        scale = lax.rsqrt(jnp.mean(value * value, axis=-1, keepdims=True) + EPS)
        norm[chunk, :] = (value * scale * mgain[...]).astype(BF16)
        weights.step(18 + t)

    @pl.loop(26, 36)
    def _(n):
        weights.step(n)

    wts[sp] = wown[...]
    both = jnp.dot(norm[...], wts[:, :, 0:768].reshape(2048, 768), preferred_element_type=F32)
    gate, up = both[:, 0:384], both[:, 384:768]
    hid[...] = (gate / (1.0 + jnp.exp(-gate)) * up).astype(BF16)

    @pl.loop(0, 8)
    def _(j):
        down = wts[pl.ds(j * 8, 8), :, 768:1152].reshape(256, 384)
        value = lax.dot_general(hid[...], down, (((1,), (1,)), ((), ())), preferred_element_type=F32)
        part[:, :, pl.ds(pl.multiple_of(j * 256, 256), 256)] = value.astype(BF16).reshape(8, 32, 256)

    latents.drain()

    @pl.loop(0, 64)
    def _(o):
        @pl.when(o != sp)
        def _():
            remote(lat.at[core, o], lat.at[core, o], p_send.at[o], p_recv.at[o], partner).wait_send()

    for i in (2, 1, 3, 0):
        x_to = rem(xx + i, 4)
        remote(part.at[2 * x_to + other], pbuf.at[x_to], s_send.at[i], s_recv.at[i], partner).start()
    ready = None
    for i, dev in ((2, x_far), (1, x_up), (3, x_dn)):
        x_to = rem(xx + i, 4)
        remote(pbuf.at[x_to], pbuf.at[x_to], s_send.at[i], s_recv.at[i], partner).wait_recv()
        sbuf[i - 1] = (part[2 * x_to + core].astype(F32) + pbuf[x_to].astype(F32)).astype(BF16)
        if ready is not None:
            ready.start()
        ready = remote(sbuf.at[i - 1], rbuf.at[i - 1], s_send.at[3 + i], s_recv.at[3 + i], dev)
    remote(pbuf.at[xx], pbuf.at[xx], s_send.at[0], s_recv.at[0], partner).wait_recv()
    summed = part[tp].astype(F32) + pbuf[xx].astype(F32)
    ready.start()
    weights.drain()
    for i in (1, 3, 2):
        remote(rbuf.at[i - 1], rbuf.at[i - 1], s_send.at[3 + i], s_recv.at[3 + i], partner).wait_recv()
        summed = summed + rbuf[i - 1].astype(F32)
    out[...] = (rows[tp].astype(F32) + 0.5 * summed).astype(BF16)

    for i in range(7):
        remote(att.at[tp], att.at[tp], a_send.at[i], a_recv.at[tp], partner).wait_send()
        remote(rbuf.at[0], rbuf.at[0], s_send.at[i], s_recv.at[i], partner).wait_send()
    for i in (0, 1, 2, 5, 6):
        remote(wout.at[tp], wout.at[tp], o_send.at[i], o_recv.at[tp], partner).wait_send()
    for i in (3, 4, 7, 8):
        remote(wout.at[tp, top], wout.at[tp, top], o_send.at[i], o_recv.at[tp], partner).wait_send()


def rotate(values, cosine, sine):
    first, second = values[:, :16], values[:, 16:]
    return jnp.concatenate([first * cosine - second * sine, first * sine + second * cosine], axis=-1)


def shards(
    residual_in, query_lean, query_broad, latent, rope_key, latent_gain, key_up_lean, key_up_broad, value_up_lean,
    value_up_broad, out_lean, out_broad, attn_gain, mlp_gain, gate_weight, up_weight, down_weight,
):
    tokens = latent.shape[0]
    positions = lax.axis_index("sp") * tokens + jnp.arange(tokens, dtype=jnp.int32)
    freqs = THETA ** (-2.0 * jnp.arange(16, dtype=F32) / 32)
    angle = positions.astype(F32)[:, None] * freqs[None, :]
    cosine, sine = jnp.cos(angle), jnp.sin(angle)

    def rounded(v):
        return rotate(v.astype(F32), cosine, sine).astype(BF16)

    wide = latent.astype(F32)
    normed = (
        wide * lax.rsqrt(jnp.mean(wide * wide, axis=-1, keepdims=True) + EPS) * latent_gain
    ).astype(BF16)
    rot = rounded(rope_key)
    turned = rot.reshape(2, HALF, 2, 16).transpose(0, 3, 2, 1).reshape(2, 16, 256)
    pieces = jnp.concatenate([normed.reshape(2, HALF, 256), turned], axis=1)
    broad, lean = query_broad[:, 0], query_lean[:, 0]
    pad = functools.partial(jnp.zeros, dtype=BF16)
    queries = jnp.concatenate(
        [
            jnp.concatenate([broad[:, :128], pad((tokens, 64)), rounded(broad[:, 128:]), pad((tokens, 32))], axis=1),
            jnp.concatenate([pad((tokens, 128)), lean[:, :64], rounded(lean[:, 64:]), pad((tokens, 32))], axis=1),
        ],
        axis=0,
    )
    vmem = pl.BlockSpec(memory_space=pltpu.VMEM)
    hbm = pl.BlockSpec(memory_space=pl.ANY)
    sems = pltpu.SemaphoreType.DMA
    scratch = [
        pltpu.VMEM((2, 64, PIECE, 256), BF16),
        pltpu.VMEM((64, 32, 1152), BF16),
        pltpu.VMEM((8, 192, 2048), BF16),
        pltpu.VMEM((8, 32, 2048), BF16),
        pltpu.VMEM((8, 192, 256), BF16),
        pltpu.VMEM((256, 512), BF16),
        pltpu.VMEM((256, 256), BF16),
        pltpu.VMEM((192, 256), BF16),
        pltpu.VMEM((32, 256), BF16),
        pltpu.VMEM((1, 512), F32),
        pltpu.VMEM((1, 512), F32),
        pltpu.VMEM((192, 256), F32),
        pltpu.VMEM((8, 256, 192), BF16),
        pltpu.VMEM((256, 2048), F32),
        pltpu.VMEM((256, 2048), BF16),
        pltpu.VMEM((256, 384), BF16),
        pltpu.VMEM((8, 32, 2048), BF16),
        pltpu.VMEM((4, 32, 2048), BF16),
        pltpu.VMEM((3, 32, 2048), BF16),
        pltpu.VMEM((3, 32, 2048), BF16),
        pltpu.VMEM((32, 1152), BF16),
        sems((64,)), sems((8,)), sems((28,)), sems((32,)), sems((64,)), sems((64,)),
        sems((64,)), sems((8,)), sems((28,)), sems((32,)),
        sems((3,)), sems((9,)), sems((12,)), sems((7,)), sems((8,)), sems((7,)), sems((8,)), sems((7,)), sems((7,)),
    ]
    return pl.pallas_call(
        kernel,
        out_shape=jax.ShapeDtypeStruct((32, 2048), BF16),
        in_specs=[vmem] * 6 + [hbm] * 3 + [vmem] * 5,
        out_specs=vmem,
        scratch_shapes=scratch,
        compiler_params=pltpu.CompilerParams(
            collective_id=0, has_side_effects=True, vmem_limit_bytes=60 * 1024 * 1024
        ),
    )(
        pieces, queries, key_up_broad[:, 0], key_up_lean[:, 0], value_up_broad[:, 0], value_up_lean[:, 0],
        out_broad[0], out_lean[0], residual_in, attn_gain[None], mlp_gain[None], gate_weight, up_weight, down_weight,
    )


def solution(mesh):
    in_specs = (
        P(("sp", "tp"), None), P("sp", "tp", None), P("sp", "tp", None), P("sp", None), P("sp", None), P(),
        P(None, "tp", None), P(None, "tp", None), P(None, "tp", None), P(None, "tp", None),
        P("tp", None, None), P("tp", None, None), P(), P(), P("sp", "tp"), P("sp", "tp"), P("tp", "sp"),
    )
    return jax.shard_map(
        shards, mesh=mesh, in_specs=in_specs, out_specs=P(("sp", "tp"), None), check_vma=False
    )
```

```python
import jax
import jax.numpy as jnp
from jax import lax
from jax.experimental import pallas as pl
from jax.experimental.pallas import tpu as pltpu
from jax.sharding import PartitionSpec as P

MESH = pl.DeviceIdType.MESH
THETA = 10000.0
EPS = 1e-06
NEGATIVE = -1e30
LOG2E = 1.4426950408889634
RING = 8
F32 = jnp.float32
BF16 = jnp.bfloat16

HALF = 128
PIECE = HALF + 16


def rem(v, n):
    return lax.rem(v, jnp.int32(n))


def div(v, n):
    return lax.div(v, jnp.int32(n))


def kernel(
    latent, lgain, rope, qb, ql, cosine, sine, kb, kl, vb, vl, ob, ol, resid, again, mgain, gate_w, up_w, down_w,
    out,
    pieces, score, value, most, lat, wts, wout, rows, att, qt, kup, vupt, spread, peak, total, accum, att_t, hs, norm, hid, part, pbuf, sbuf, rbuf, wown,
    l_recv, w_recv, p_recv, first, plus, minus, p_send,
    loc, o_send, o_recv, r_send, r_recv, a_send, a_recv, s_send, s_recv,
):
    sp = lax.axis_index("sp")
    tp = lax.axis_index("tp")
    core = rem(tp, 2)
    xx = div(tp, 2)
    other = 1 - core
    sa = 1 + 7 * core
    sb = 8 - 7 * core
    a = rem(lax.div(sp, sa), RING)
    b = rem(lax.div(sp, sb), RING)

    def at(i, j):
        return rem(i + 16, RING) * sa + rem(j + 16, RING) * sb

    def turned(i, j):
        return rem(i + 16, RING) * sb + rem(j + 16, RING) * sa

    def rel(k):
        return div(k + 1, 2) * (1 - 2 * rem(k, 2))

    a_up, a_dn, b_up, b_dn = (
        (at(a + 1, b), tp), (at(a - 1, b), tp), (at(a, b + 1), tp), (at(a, b - 1), tp)
    )
    partner = (sp, 2 * xx + other)

    def across(step):
        return 2 * rem(xx + step, 4) + core

    x_up, x_far, x_dn = (sp, across(1)), (sp, across(2)), (sp, across(3))

    def remote(src, dst, ssem, rsem, dev):
        return pltpu.make_async_remote_copy(
            src_ref=src, dst_ref=dst, send_sem=ssem, recv_sem=rsem, device_id=dev, device_id_type=MESH
        )

    own_b = pltpu.make_async_copy(ob, wout.at[tp, pl.ds(0, 128)], loc.at[0])
    own_l = pltpu.make_async_copy(ol, wout.at[tp, pl.ds(128, 64)], loc.at[1])
    own_r = pltpu.make_async_copy(resid, rows.at[tp], loc.at[2])
    own_b.start()
    own_l.start()
    own_r.start()

    barrier = pltpu.get_barrier_semaphore()
    for dev in (a_up, a_dn, b_up, b_dn, partner, x_up, x_far, x_dn):
        pl.semaphore_signal(barrier, inc=1, device_id=dev, device_id_type=MESH)

    def rotated(ref, start):
        low, high = ref[start : start + 16, :].astype(F32), ref[start + 16 : start + 32, :].astype(F32)
        co, si = cosine[...], sine[...]
        return (low * co - high * si).astype(BF16), (low * si + high * co).astype(BF16)

    wide = latent[...].astype(F32)
    wide = (wide * lax.rsqrt(jnp.mean(wide * wide, axis=-1, keepdims=True) + EPS) * lgain[...]).astype(BF16)
    low, high = rotated(rope, 0)
    for h in range(2):
        pieces[h, 0:HALF, :] = wide[h * HALF : (h + 1) * HALF]
        pieces[h, HALF:PIECE, 0:HALF] = low[:, h * HALF : (h + 1) * HALF]
        pieces[h, HALF:PIECE, HALF:256] = high[:, h * HALF : (h + 1) * HALF]
    qt[...] = jnp.zeros_like(qt)
    qt[0:128, 0:256] = qb[0:128, :]
    qt[128:192, 256:512] = ql[0:64, :]
    for ref, start, at_column in ((qb, 128, 0), (ql, 64, 256)):
        low, high = rotated(ref, start)
        qt[192:208, at_column : at_column + 256] = low
        qt[208:224, at_column : at_column + 256] = high

    pl.semaphore_wait(barrier, 8)

    class Stream:
        def __init__(self, own, slot, pair, recv, fresh):
            self.own, self.slot, self.pair, self.recv, self.fresh = own, slot, pair, recv, fresh

        def go(self, src, o, ssem, n, dev):
            remote(src, self.slot(o), ssem, self.recv.at[n], dev).start()

        def free(self, sem, when=True):
            if when is True:
                remote(self.slot(0), self.slot(0), sem, self.recv.at[0], partner).wait_send()
            else:
                pl.when(when)(lambda: self.free(sem))

        def start(self):
            for index, n, dev in ((0, 1, a_up), (7, 2, a_dn)):
                if not self.fresh:
                    self.free(first.at[index])
                self.go(self.own, sp, first.at[index], n, dev)

        def spread(self, k, src=None):
            o = at(a + rel(k), b)
            src = self.slot(o) if src is None else src
            for sems, dev in ((plus, b_up), (minus, b_dn)):
                if not self.fresh:
                    self.free(sems.at[k])
                self.go(src, o, sems.at[k], k + 8, dev)

        def near(self, k):
            o = at(a + rel(k), b)
            remote(self.slot(o), self.slot(o), first.at[0], self.recv.at[k], partner).wait_recv()

            @pl.when((rem(k, 2) == 1) & (k < 7))
            def _():
                if not self.fresh:
                    self.free(first.at[k])
                self.go(self.slot(o), o, first.at[k], k + 2, a_up)

            @pl.when((rem(k, 2) == 0) & (k < 6))
            def _():
                if not self.fresh:
                    self.free(first.at[k])
                self.go(self.slot(o), o, first.at[k], k + 2, a_dn)

        def far(self, n):
            kp, km, d = ring_step(n)
            k = rem(n, 8)
            op, om = at(a + rel(kp), b - d), at(a + rel(km), b + d)
            remote(self.pair, self.pair, first.at[0], self.recv.at[n], partner).wait_recv()

            @pl.when(n < 28)
            def _():
                self.free(plus.at[k])
                self.go(self.slot(op), op, plus.at[k], n + 8, b_up)

            @pl.when((n < 24) | ((n >= 28) & (n < 32)))
            def _():
                self.free(minus.at[k])
                self.go(self.slot(om), om, minus.at[k], jnp.where(n < 24, n + 8, n + 4), b_dn)

            return k, op, om

    def give(n, o):
        remote(lat.at[core, o], lat.at[core, o], p_send.at[rem(n, 8)], p_recv.at[n], partner).start()

    two = lat.at[0, pl.ds(0, 2)]

    def given_free(n, count):
        ref = two if count == 2 else lat.at[0, 0]
        remote(ref, ref, p_send.at[rem(n, 8)], p_recv.at[0], partner).wait_send()

    def ring_step(n):
        last = div(n, 32)
        kp = rem(n, 8)
        return kp, kp + 4 * last, div(n, 8)

    latents = Stream(pieces.at[core], lambda o: lat.at[core, o], two, l_recv, True)
    weights = Stream(wown, lambda o: wts.at[o], wts.at[pl.ds(0, 2)], w_recv, False)

    def latent_near(k):
        latents.near(k)
        latents.spread(k)
        give(k, at(a + rel(k), b))

    def latent_far(n):
        k, op, om = latents.far(n)

        @pl.when(n >= 16)
        def _():
            given_free(n, 2)

        @pl.when((n > 8) & (n < 16))
        def _():
            given_free(n, 1)

        give(n, op)
        give(n, om)

    latents.start()
    latents.spread(jnp.int32(0), pieces.at[core])

    own_r.wait()
    for i, dev in enumerate((partner, x_up, x_dn, x_far)):
        remote(rows.at[tp], rows.at[tp], r_send.at[i], r_recv.at[tp], dev).start()
    own_b.wait()
    own_l.wait()
    for i, dev in enumerate((partner, x_up, x_dn)):
        remote(wout.at[tp], wout.at[tp], o_send.at[i], o_recv.at[tp], dev).start()

    def share_rows():
        for i in (1, 2, 3):
            t = across(i)
            remote(rows.at[t], rows.at[t], r_send.at[3 + i], r_recv.at[t], partner).wait_recv()
            remote(rows.at[t], rows.at[t], r_send.at[3 + i], r_recv.at[t], partner).start()

    top, low = pl.ds(0, 96), pl.ds(96, 96)

    def share_near():
        for i, t, rest, dev in ((3, across(3), top, x_up), (4, across(1), low, x_dn)):
            remote(wout.at[t], wout.at[t], o_send.at[i], o_recv.at[t], partner).wait_recv()
            far = 8 if i == 3 else 9
            remote(wout.at[t, rest], wout.at[t, rest], o_send.at[i], o_recv.at[far], dev).start()
            remote(wout.at[t], wout.at[t], o_send.at[i + 2], o_recv.at[t], partner).start()

    def share_far():
        t = across(2)
        for i, rest in ((8, top), (9, low)):
            remote(wout.at[t, rest], wout.at[t, rest], o_send.at[0], o_recv.at[i], partner).wait_recv()
            remote(wout.at[t, rest], wout.at[t, rest], o_send.at[i - 1], o_recv.at[i + 2], partner).start()

    kup[...] = jnp.zeros_like(kup)
    kup[:, 0:128] = kb[...]
    kup[:, 128:192] = kl[...].T
    vupt[0:128, :] = vb[...].T
    vupt[128:192, :] = vl[...]
    spread[...] = (
        lax.broadcasted_iota(jnp.int32, (32, 256), 1) == lax.broadcasted_iota(jnp.int32, (32, 256), 0) + 192
    ).astype(F32).astype(BF16)
    wown[...] = jnp.zeros_like(wown)
    wown[:, 0:352] = gate_w[...]
    wown[:, 384:736] = up_w[...]
    wown[:, 768:1120] = down_w[...]

    column = lax.broadcasted_iota(jnp.int32, (1, 512), 1)
    factor = jnp.where(column < 256, LOG2E * 160 ** (-0.5), LOG2E * 96 ** (-0.5)).astype(F32)

    def project(halves):
        rows_of = jnp.concatenate([h[0:HALF, :] for h in halves], axis=0)
        turned_rot = jnp.concatenate(
            [
                jnp.concatenate([h[HALF:PIECE, 0:HALF] for h in halves], axis=1),
                jnp.concatenate([h[HALF:PIECE, HALF:256] for h in halves], axis=1),
            ],
            axis=0,
        )
        keys = jnp.dot(rows_of, kup[...], preferred_element_type=F32) + lax.dot_general(
            turned_rot, spread[...], (((0,), (0,)), ((), ())), preferred_element_type=F32
        )
        values = lax.dot_general(
            vupt[...], rows_of, (((1,), (1,)), ((), ())), preferred_element_type=F32
        )
        return keys.astype(BF16), values.astype(BF16)

    def fold(halves, blocks):
        keys, values = project(halves)
        scores = jnp.dot(keys, qt[...], preferred_element_type=F32) * factor
        if blocks is None:
            seen = lax.broadcasted_iota(jnp.int32, scores.shape, 0) <= (
                lax.broadcasted_iota(jnp.int32, scores.shape, 1) & 255
            )
            scores = jnp.where(seen, scores, NEGATIVE)
        else:
            scores = jnp.concatenate(
                [
                    scores[i * HALF : (i + 1) * HALF] + jnp.where(o <= sp, 0.0, NEGATIVE).astype(F32)
                    for i, o in enumerate(blocks)
                ],
                axis=0,
            )
        old = peak[...]
        new = jnp.maximum(old, jnp.max(scores, axis=0, keepdims=True))
        shrink = jnp.exp2(old - new)
        wt = jnp.exp2(scores - new)
        peak[...] = new
        total[...] = total[...] * shrink + jnp.sum(wt, axis=0, keepdims=True)
        wt = wt.astype(BF16)
        accum[0:128, :] = accum[0:128, :] * shrink[:, 0:256] + jnp.dot(
            values[0:128], wt[:, 0:256], preferred_element_type=F32
        )
        accum[128:192, :] = accum[128:192, :] * shrink[:, 256:512] + jnp.dot(
            values[128:192], wt[:, 256:512], preferred_element_type=F32
        )

    def begin(halves, slot):
        keys, vals = project(halves)
        raw = jnp.dot(keys, qt[...], preferred_element_type=F32)
        score[slot] = raw
        value[slot] = vals
        for i in range(4):
            most[slot, i : i + 1, :] = jnp.max(raw[i * HALF : (i + 1) * HALF], axis=0, keepdims=True)

    def finish(blocks, there, slot):
        hidden = [jnp.where((o <= sp) & there, 0.0, NEGATIVE).astype(F32) for o in blocks]
        old = peak[...]
        new = old
        for i in range(4):
            new = jnp.maximum(new, most[slot, i : i + 1, :] * factor + hidden[i])
        shrink = jnp.exp2(old - new)
        peak[...] = new
        parts = [
            jnp.exp2(score[slot, i * HALF : (i + 1) * HALF, :] * factor - (new - hidden[i])) for i in range(4)
        ]
        total[...] = total[...] * shrink + jnp.sum(
            (parts[0] + parts[1]) + (parts[2] + parts[3]), axis=0, keepdims=True
        )
        wt = jnp.concatenate([p.astype(BF16) for p in parts], axis=0)
        accum[0:128, :] = accum[0:128, :] * shrink[:, 0:256] + jnp.dot(
            value[slot, 0:128, :], wt[:, 0:256], preferred_element_type=F32
        )
        accum[128:192, :] = accum[128:192, :] * shrink[:, 256:512] + jnp.dot(
            value[slot, 128:192, :], wt[:, 256:512], preferred_element_type=F32
        )

    score[...] = jnp.zeros_like(score)
    value[...] = jnp.zeros_like(value)
    most[...] = jnp.zeros_like(most)
    peak[...] = jnp.full_like(peak, NEGATIVE)
    total[...] = jnp.zeros_like(total)
    accum[...] = jnp.zeros_like(accum)
    fold([pieces.at[0], pieces.at[1]], None)

    def given(n, count):
        ref = two if count == 2 else lat.at[0, 0]
        remote(ref, ref, p_send.at[0], p_recv.at[n], partner).wait_recv()

    def blocks_of(n):
        kp, km, d = ring_step(n)
        return (
            at(a + rel(kp), b - d), at(a + rel(km), b + d), turned(b + rel(kp), a - d), turned(b + rel(km), a + d)
        )

    def halves_of(o):
        return [lat.at[core, o[0]], lat.at[core, o[1]], lat.at[other, o[2]], lat.at[other, o[3]]]

    def least(o):
        return jnp.minimum(jnp.minimum(o[0], o[1]), jnp.minimum(o[2], o[3]))

    def near_blocks(n):
        return at(a + rel(n), b), turned(b + rel(n), a)

    @pl.loop(0, 3)
    def _(j):
        n = 1 + 2 * j
        latent_near(n)
        latent_near(n + 1)

        @pl.when(j > 0)
        def _():
            given(n - 2, 1)
            given(n - 1, 1)
            one, two_ = near_blocks(n - 2), near_blocks(n - 1)
            o = (one[0], two_[0], one[1], two_[1])

            @pl.when(least(o) <= sp)
            def _():
                begin(halves_of(o), 0)
                finish(o, sp >= 0, 0)

    latent_near(jnp.int32(7))
    latent_far(jnp.int32(8))
    given(jnp.int32(5), 1)
    given(jnp.int32(6), 1)
    one, two_ = near_blocks(jnp.int32(5)), near_blocks(jnp.int32(6))
    last_near = (one[0], two_[0], one[1], two_[1])
    begin(halves_of(last_near), 1)
    latent_far(jnp.int32(9))
    latent_far(jnp.int32(10))
    given(jnp.int32(7), 1)
    seventh = near_blocks(jnp.int32(7))

    @pl.when(jnp.minimum(seventh[0], seventh[1]) <= sp)
    def _():
        fold([lat.at[core, seventh[0]], lat.at[other, seventh[1]]], seventh)

    @pl.loop(0, 14)
    def _(m):
        n = 8 + 2 * m

        @pl.when(n + 3 < 36)
        def _():
            latent_far(n + 3)

        @pl.when(n + 4 < 36)
        def _():
            latent_far(n + 4)

        @pl.when(m == 1)
        def _():
            weights.start()

        @pl.when((m == 4) | (m == 6) | (m == 8))
        def _():
            weights.near(m - 3)
            weights.near(m - 2)

        @pl.when(m == 10)
        def _():
            weights.near(m - 3)
            weights.spread(jnp.int32(0), wown)

            @pl.loop(1, 8)
            def _(k):
                weights.spread(k)

        @pl.when(m == 12)
        def _():
            weights.far(jnp.int32(8))

        @pl.when(m == 13)
        def _():
            weights.far(jnp.int32(9))
            weights.far(jnp.int32(10))

        @pl.when(m == 5)
        def _():
            share_rows()

        @pl.when(m == 9)
        def _():
            share_near()

        now, after = blocks_of(n), blocks_of(n + 1)
        past = blocks_of(n - 1)
        before = [jnp.where(m == 0, o, p) for o, p in zip(last_near, past)]
        given(n, 2)
        given(n + 1, 2)

        @pl.when(jnp.minimum(jnp.minimum(least(before), least(now)), least(after)) <= sp)
        def _():
            begin(halves_of(now), 0)
            finish(before, m >= 0, 1)
            begin(halves_of(after), 1)
            finish(now, m >= 0, 0)

    finish(blocks_of(jnp.int32(35)), sp >= 0, 1)

    result = accum[...]
    att[tp, 0:128, :] = (result[0:128] / total[:, 0:256]).astype(BF16)
    att[tp, 128:192, :] = (result[128:192] / total[:, 256:512]).astype(BF16)

    weights.far(jnp.int32(11))

    for i, dev in enumerate((x_far, x_up, x_dn, partner)):
        remote(att.at[tp], att.at[tp], a_send.at[i], a_recv.at[tp], dev).start()

    share_far()

    @pl.loop(12, 14)
    def _(n):
        weights.far(n)

    for i in (1, 3, 2):
        t = across(i)
        remote(att.at[t], att.at[t], a_send.at[0], a_recv.at[t], partner).wait_recv()
        remote(att.at[t], att.at[t], a_send.at[3 + i], a_recv.at[t], partner).start()
        weights.far(jnp.int32({1: 14, 3: 15, 2: 16}[i]))

    weights.far(jnp.int32(17))

    for i in (0, 1, 2, 3):
        t = 2 * rem(xx + i, 4) + other
        remote(att.at[t], att.at[t], a_send.at[0], a_recv.at[t], partner).wait_recv()
        remote(rows.at[t], rows.at[t], r_send.at[0], r_recv.at[t], partner).wait_recv()
        if i == 2:
            for j, rest in ((10, top), (11, low)):
                remote(wout.at[t, rest], wout.at[t, rest], o_send.at[0], o_recv.at[j], partner).wait_recv()
        else:
            remote(wout.at[t], wout.at[t], o_send.at[0], o_recv.at[t], partner).wait_recv()

    @pl.loop(0, 8)
    def _(t):
        att_t[t] = att[t].T

    @pl.loop(0, 8)
    def _(j):
        cols = pl.ds(pl.multiple_of(j * 256, 256), 256)
        acc = jnp.dot(att_t[0], wout[0, :, cols], preferred_element_type=F32)
        for t in range(1, 8):
            acc = acc + jnp.dot(att_t[t], wout[t, :, cols], preferred_element_type=F32)
        hs[:, cols] = acc
        weights.far(18 + j)

    for i in range(7):
        remote(rows.at[tp], rows.at[tp], r_send.at[i], r_recv.at[tp], partner).wait_send()

    @pl.loop(0, 8)
    def _(t):
        chunk = pl.ds(pl.multiple_of(t * 32, 32), 32)
        value = hs[chunk, :]
        scale = lax.rsqrt(jnp.mean(value * value, axis=-1, keepdims=True) + EPS)
        mixed = (rows[t].astype(F32) + value * scale * again[...]).astype(BF16)
        rows[t] = mixed
        value = mixed.astype(F32)
        scale = lax.rsqrt(jnp.mean(value * value, axis=-1, keepdims=True) + EPS)
        norm[chunk, :] = (value * scale * mgain[...]).astype(BF16)
        weights.far(26 + t)

    weights.far(jnp.int32(34))
    weights.far(jnp.int32(35))

    wts[sp] = wown[...]
    both = jnp.dot(norm[...], wts[:, :, 0:768].reshape(2048, 768), preferred_element_type=F32)
    gate, up = both[:, 0:384], both[:, 384:768]
    hid[...] = (gate / (1.0 + jnp.exp(-gate)) * up).astype(BF16)

    @pl.loop(0, 2)
    def _(j):
        down = wts[pl.ds(j * 32, 32), :, 768:1152].reshape(1024, 384)
        block = lax.dot_general(hid[...], down, (((1,), (1,)), ((), ())), preferred_element_type=F32)
        part[:, :, pl.ds(pl.multiple_of(j * 1024, 1024), 1024)] = block.astype(BF16).reshape(8, 32, 1024)

    for i in (2, 1, 3, 0):
        x_to = rem(xx + i, 4)
        remote(part.at[2 * x_to + other], pbuf.at[x_to], s_send.at[i], s_recv.at[i], partner).start()
    ready = None
    for i, dev in ((2, x_far), (1, x_up), (3, x_dn)):
        x_to = rem(xx + i, 4)
        remote(pbuf.at[x_to], pbuf.at[x_to], s_send.at[i], s_recv.at[i], partner).wait_recv()
        sbuf[i - 1] = (part[2 * x_to + core].astype(F32) + pbuf[x_to].astype(F32)).astype(BF16)
        if ready is not None:
            ready.start()
        ready = remote(sbuf.at[i - 1], rbuf.at[i - 1], s_send.at[3 + i], s_recv.at[3 + i], dev)
    remote(pbuf.at[xx], pbuf.at[xx], s_send.at[0], s_recv.at[0], partner).wait_recv()
    summed = part[tp].astype(F32) + pbuf[xx].astype(F32)
    ready.start()
    @pl.loop(0, 8)
    def _(n):
        for sems in (plus, minus):
            weights.free(sems.at[n])
        given_free(n, 2)

        @pl.when(n != 6)
        def _():
            weights.free(first.at[n])

    for i in (1, 3, 2):
        remote(rbuf.at[i - 1], rbuf.at[i - 1], s_send.at[3 + i], s_recv.at[3 + i], partner).wait_recv()
        summed = summed + rbuf[i - 1].astype(F32)
    out[...] = (rows[tp].astype(F32) + 0.5 * summed).astype(BF16)

    for i in range(7):
        remote(att.at[tp], att.at[tp], a_send.at[i], a_recv.at[tp], partner).wait_send()
        remote(rbuf.at[0], rbuf.at[0], s_send.at[i], s_recv.at[i], partner).wait_send()
    for i in (0, 1, 2, 5, 6):
        remote(wout.at[tp], wout.at[tp], o_send.at[i], o_recv.at[tp], partner).wait_send()
    for i in (3, 4, 7, 8):
        remote(wout.at[tp, top], wout.at[tp, top], o_send.at[i], o_recv.at[tp], partner).wait_send()


def shards(
    residual_in, query_lean, query_broad, latent, rope_key, latent_gain, key_up_lean, key_up_broad, value_up_lean,
    value_up_broad, out_lean, out_broad, attn_gain, mlp_gain, gate_weight, up_weight, down_weight,
):
    tokens = latent.shape[0]
    positions = lax.axis_index("sp") * tokens + jnp.arange(tokens, dtype=jnp.int32)
    freqs = THETA ** (-2.0 * jnp.arange(16, dtype=F32) / 32)
    angle = freqs[:, None] * positions.astype(F32)[None, :]
    vmem = pl.BlockSpec(memory_space=pltpu.VMEM)
    hbm = pl.BlockSpec(memory_space=pl.ANY)
    sems = pltpu.SemaphoreType.DMA
    scratch = [
        pltpu.VMEM((2, PIECE, 256), BF16),
        pltpu.VMEM((2, 512, 512), F32),
        pltpu.VMEM((2, 192, 512), BF16),
        pltpu.VMEM((2, 8, 512), F32),
        pltpu.VMEM((2, 64, PIECE, 256), BF16),
        pltpu.VMEM((64, 32, 1152), BF16),
        pltpu.VMEM((8, 192, 2048), BF16),
        pltpu.VMEM((8, 32, 2048), BF16),
        pltpu.VMEM((8, 192, 256), BF16),
        pltpu.VMEM((256, 512), BF16),
        pltpu.VMEM((256, 256), BF16),
        pltpu.VMEM((192, 256), BF16),
        pltpu.VMEM((32, 256), BF16),
        pltpu.VMEM((1, 512), F32),
        pltpu.VMEM((1, 512), F32),
        pltpu.VMEM((192, 256), F32),
        pltpu.VMEM((8, 256, 192), BF16),
        pltpu.VMEM((256, 2048), F32),
        pltpu.VMEM((256, 2048), BF16),
        pltpu.VMEM((256, 384), BF16),
        pltpu.VMEM((8, 32, 2048), BF16),
        pltpu.VMEM((4, 32, 2048), BF16),
        pltpu.VMEM((3, 32, 2048), BF16),
        pltpu.VMEM((3, 32, 2048), BF16),
        pltpu.VMEM((32, 1152), BF16),
        sems((36,)), sems((36,)), sems((36,)), sems((8,)), sems((8,)), sems((8,)), sems((8,)),
        sems((3,)), sems((9,)), sems((12,)), sems((7,)), sems((8,)), sems((7,)), sems((8,)), sems((7,)), sems((7,)),
    ]
    return pl.pallas_call(
        kernel,
        out_shape=jax.ShapeDtypeStruct((32, 2048), BF16),
        in_specs=[vmem] * 11 + [hbm] * 3 + [vmem] * 5,
        out_specs=vmem,
        scratch_shapes=scratch,
        compiler_params=pltpu.CompilerParams(
            collective_id=0, has_side_effects=True, vmem_limit_bytes=60 * 1024 * 1024
        ),
    )(
        latent, latent_gain[None], rope_key.T, query_broad[:, 0].T, query_lean[:, 0].T, jnp.cos(angle), jnp.sin(angle),
        key_up_broad[:, 0], key_up_lean[:, 0].T, value_up_broad[:, 0], value_up_lean[:, 0].T,
        out_broad[0], out_lean[0], residual_in, attn_gain[None], mlp_gain[None], gate_weight, up_weight, down_weight.T,
    )


def solution(mesh):
    in_specs = (
        P(("sp", "tp"), None), P("sp", "tp", None), P("sp", "tp", None), P("sp", None), P("sp", None), P(),
        P(None, "tp", None), P(None, "tp", None), P(None, "tp", None), P(None, "tp", None),
        P("tp", None, None), P("tp", None, None), P(), P(), P("sp", "tp"), P("sp", "tp"), P("tp", "sp"),
    )
    return jax.shard_map(
        shards, mesh=mesh, in_specs=in_specs, out_specs=P(("sp", "tp"), None), check_vma=False
    )
```

```python
import jax
import jax.numpy as jnp
from jax import lax
from jax.experimental import pallas as pl
from jax.experimental.pallas import tpu as pltpu
from jax.sharding import PartitionSpec as P

MESH = pl.DeviceIdType.MESH
THETA = 10000.0
EPS = 1e-06
NEGATIVE = -1e30
LOG2E = 1.4426950408889634
RING = 8
F32 = jnp.float32
BF16 = jnp.bfloat16

HALF = 128
PIECE = HALF + 16


def rem(v, n):
    return lax.rem(v, jnp.int32(n))


def div(v, n):
    return lax.div(v, jnp.int32(n))


def kernel(
    *args,
):
    inputs, (ob, ol, resid, out), rest = args[:16], args[16:20], args[20:]
    held, rest, in_sem = rest[:16], rest[16:-1], rest[-1]
    run(inputs, held, in_sem, ob, ol, resid, out, *rest)


def run(
    inputs, held, in_sem, ob, ol, resid, out,
    pieces, score, value, most, lat, wts, wout, rows, att, qt, kup, vupt, spread, peak, total, accum, att_t, hs, norm, hid, part, pbuf, sbuf, rbuf, cbuf, wown,
    l_recv, w_recv, p_recv, first, plus, minus, p_send,
    loc, o_send, o_recv, r_send, r_recv, a_send, a_recv, s_send, s_recv,
):
    sp = lax.axis_index("sp")
    tp = lax.axis_index("tp")
    core = rem(tp, 2)
    xx = div(tp, 2)
    other = 1 - core
    sa = 1 + 7 * core
    sb = 8 - 7 * core
    a = rem(lax.div(sp, sa), RING)
    b = rem(lax.div(sp, sb), RING)

    def at(i, j):
        return rem(i + 16, RING) * sa + rem(j + 16, RING) * sb

    def turned(i, j):
        return rem(i + 16, RING) * sb + rem(j + 16, RING) * sa

    def rel(k):
        return div(k + 1, 2) * (1 - 2 * rem(k, 2))

    a_up, a_dn, b_up, b_dn = (
        (at(a + 1, b), tp), (at(a - 1, b), tp), (at(a, b + 1), tp), (at(a, b - 1), tp)
    )
    a_up2, a_dn2 = (at(a + 2, b), tp), (at(a - 2, b), tp)
    partner = (sp, 2 * xx + other)

    def across(step):
        return 2 * rem(xx + step, 4) + core

    x_up, x_far, x_dn = (sp, across(1)), (sp, across(2)), (sp, across(3))

    def remote(src, dst, ssem, rsem, dev):
        return pltpu.make_async_remote_copy(
            src_ref=src, dst_ref=dst, send_sem=ssem, recv_sem=rsem, device_id=dev, device_id_type=MESH
        )

    latent, lgain, rope, cosine, sine, qb, ql, kb, kl, vb, vl, again, mgain, gate_w, up_w, down_w = held
    barrier = pltpu.get_barrier_semaphore()
    for dev in (a_up, a_dn, b_up, b_dn, partner, x_up, x_far, x_dn, a_up2, a_dn2):
        pl.semaphore_signal(barrier, inc=1, device_id=dev, device_id_type=MESH)
    loads = [pltpu.make_async_copy(src, dst, in_sem.at[i]) for i, (src, dst) in enumerate(zip(inputs, held))]
    for load in loads:
        load.start()

    own_b = pltpu.make_async_copy(ob, wout.at[tp, pl.ds(0, 128)], loc.at[0])
    own_l = pltpu.make_async_copy(ol, wout.at[tp, pl.ds(128, 64)], loc.at[1])
    own_r = pltpu.make_async_copy(resid, rows.at[tp], loc.at[2])
    own_b.start()
    own_l.start()
    own_r.start()

    for load in loads[:7]:
        load.wait()

    def rotated(ref, start):
        low, high = ref[start : start + 16, :].astype(F32), ref[start + 16 : start + 32, :].astype(F32)
        co, si = cosine[...], sine[...]
        return (low * co - high * si).astype(BF16), (low * si + high * co).astype(BF16)

    wide = latent[...].astype(F32)
    wide = (wide * lax.rsqrt(jnp.mean(wide * wide, axis=-1, keepdims=True) + EPS) * lgain[...]).astype(BF16)
    low, high = rotated(rope, 0)
    for h in range(2):
        pieces[h, 0:HALF, :] = wide[h * HALF : (h + 1) * HALF]
        pieces[h, HALF:PIECE, 0:HALF] = low[:, h * HALF : (h + 1) * HALF]
        pieces[h, HALF:PIECE, HALF:256] = high[:, h * HALF : (h + 1) * HALF]
    qt[128:256, :] = jnp.zeros((128, 512), BF16)
    qt[0:128, 256:512] = jnp.zeros((128, 256), BF16)
    qt[0:128, 0:256] = qb[0:128, :]
    qt[128:192, 256:512] = ql[0:64, :]
    for ref, start, at_column in ((qb, 128, 0), (ql, 64, 256)):
        low, high = rotated(ref, start)
        qt[192:208, at_column : at_column + 256] = low
        qt[208:224, at_column : at_column + 256] = high

    for load in loads[7:]:
        load.wait()
    pl.semaphore_wait(barrier, 10)

    class Stream:
        def __init__(self, own, slot, pair, recv, fresh):
            self.own, self.slot, self.pair, self.recv, self.fresh = own, slot, pair, recv, fresh

        def go(self, src, o, ssem, n, dev):
            remote(src, self.slot(o), ssem, self.recv.at[n], dev).start()

        def free(self, sem, when=True):
            if when is True:
                remote(self.slot(0), self.slot(0), sem, self.recv.at[0], partner).wait_send()
            else:
                pl.when(when)(lambda: self.free(sem))

        def start(self):
            for index, n, dev in ((0, 1, a_up), (7, 2, a_dn)):
                if not self.fresh:
                    self.free(first.at[index])
                self.go(self.own, sp, first.at[index], n, dev)

        def spread(self, k, src=None):
            o = at(a + rel(k), b)
            src = self.slot(o) if src is None else src
            for sems, dev in ((plus, b_up), (minus, b_dn)):
                if not self.fresh:
                    self.free(sems.at[k])
                self.go(src, o, sems.at[k], k + 8, dev)

        def near(self, k):
            o = at(a + rel(k), b)
            remote(self.slot(o), self.slot(o), first.at[0], self.recv.at[k], partner).wait_recv()

            @pl.when((rem(k, 2) == 1) & (k < 7))
            def _():
                if not self.fresh:
                    self.free(first.at[k])
                self.go(self.slot(o), o, first.at[k], k + 2, a_up)

            @pl.when((rem(k, 2) == 0) & (k < 6))
            def _():
                if not self.fresh:
                    self.free(first.at[k])
                self.go(self.slot(o), o, first.at[k], k + 2, a_dn)

        def far(self, n):
            kp, km, d = ring_step(n)
            k = rem(n, 8)
            op, om = at(a + rel(kp), b - d), at(a + rel(km), b + d)
            remote(self.pair, self.pair, first.at[0], self.recv.at[n], partner).wait_recv()

            @pl.when(n < 28)
            def _():
                self.free(plus.at[k])
                self.go(self.slot(op), op, plus.at[k], n + 8, b_up)

            @pl.when((n < 24) | ((n >= 28) & (n < 32)))
            def _():
                self.free(minus.at[k])
                self.go(self.slot(om), om, minus.at[k], jnp.where(n < 24, n + 8, n + 4), b_dn)

            return k, op, om

    def give(n, o):
        remote(lat.at[core, o], lat.at[core, o], p_send.at[rem(n, 8)], p_recv.at[n], partner).start()

    two = lat.at[0, pl.ds(0, 2)]

    def given_free(n, count):
        ref = two if count == 2 else lat.at[0, 0]
        remote(ref, ref, p_send.at[rem(n, 8)], p_recv.at[0], partner).wait_send()

    def ring_step(n):
        last = div(n, 32)
        kp = rem(n, 8)
        return kp, kp + 4 * last, div(n, 8)

    latents = Stream(pieces.at[core], lambda o: lat.at[core, o], two, l_recv, True)
    weights = Stream(wown, lambda o: wts.at[o], wts.at[pl.ds(0, 2)], w_recv, False)

    def latent_near(k):
        o = at(a + rel(k), b)
        remote(lat.at[core, o], lat.at[core, o], first.at[0], l_recv.at[k], partner).wait_recv()

        @pl.when((k == 1) | (k == 3))
        def _():
            latents.go(lat.at[core, o], o, first.at[k], k + 4, a_up2)

        @pl.when(k == 2)
        def _():
            latents.go(lat.at[core, o], o, first.at[k], k + 4, a_dn2)

        give(k, o)

    def latent_far(n):
        k, op, om = latents.far(n)

        @pl.when(n >= 16)
        def _():
            given_free(n, 2)

        @pl.when((n > 8) & (n < 16))
        def _():
            given_free(n, 1)

        give(n, op)
        give(n, om)

    latents.start()
    latents.go(latents.own, sp, first.at[5], 3, a_up2)
    latents.go(latents.own, sp, first.at[4], 4, a_dn2)

    own_r.wait()
    for i, dev in enumerate((partner, x_up, x_dn, x_far)):
        remote(rows.at[tp], rows.at[tp], r_send.at[i], r_recv.at[tp], dev).start()
    own_b.wait()
    own_l.wait()
    for i, dev in enumerate((partner, x_up, x_dn)):
        remote(wout.at[tp], wout.at[tp], o_send.at[i], o_recv.at[tp], dev).start()

    def share_rows():
        for i in (1, 2, 3):
            t = across(i)
            remote(rows.at[t], rows.at[t], r_send.at[3 + i], r_recv.at[t], partner).wait_recv()
            remote(rows.at[t], rows.at[t], r_send.at[3 + i], r_recv.at[t], partner).start()

    top, low = pl.ds(0, 96), pl.ds(96, 96)

    def share_near():
        for i, t, rest, dev in ((3, across(3), top, x_up), (4, across(1), low, x_dn)):
            remote(wout.at[t], wout.at[t], o_send.at[i], o_recv.at[t], partner).wait_recv()
            far = 8 if i == 3 else 9
            remote(wout.at[t, rest], wout.at[t, rest], o_send.at[i], o_recv.at[far], dev).start()
            remote(wout.at[t], wout.at[t], o_send.at[i + 2], o_recv.at[t], partner).start()

    def share_far():
        t = across(2)
        for i, rest in ((8, top), (9, low)):
            remote(wout.at[t, rest], wout.at[t, rest], o_send.at[0], o_recv.at[i], partner).wait_recv()
            remote(wout.at[t, rest], wout.at[t, rest], o_send.at[i - 1], o_recv.at[i + 2], partner).start()

    kup[...] = jnp.zeros_like(kup)
    kup[:, 0:128] = kb[...]
    kup[:, 128:192] = kl[...].T
    vupt[0:128, :] = vb[...].T
    vupt[128:192, :] = vl[...]
    spread[...] = (
        lax.broadcasted_iota(jnp.int32, (32, 256), 1) == lax.broadcasted_iota(jnp.int32, (32, 256), 0) + 192
    ).astype(F32).astype(BF16)

    column = lax.broadcasted_iota(jnp.int32, (1, 512), 1)
    factor = jnp.where(column < 256, LOG2E * 160 ** (-0.5), LOG2E * 96 ** (-0.5)).astype(F32)

    def project(halves):
        rows_of = jnp.concatenate([h[0:HALF, :] for h in halves], axis=0)
        turned_rot = jnp.concatenate(
            [
                jnp.concatenate([h[HALF:PIECE, 0:HALF] for h in halves], axis=1),
                jnp.concatenate([h[HALF:PIECE, HALF:256] for h in halves], axis=1),
            ],
            axis=0,
        )
        keys = jnp.dot(rows_of, kup[...], preferred_element_type=F32) + lax.dot_general(
            turned_rot, spread[...], (((0,), (0,)), ((), ())), preferred_element_type=F32
        )
        values = lax.dot_general(
            vupt[...], rows_of, (((1,), (1,)), ((), ())), preferred_element_type=F32
        )
        return keys.astype(BF16), values.astype(BF16)

    def fold(halves, blocks):
        keys, values = project(halves)
        scores = jnp.dot(keys, qt[...], preferred_element_type=F32) * factor
        if blocks is None:
            seen = lax.broadcasted_iota(jnp.int32, scores.shape, 0) <= (
                lax.broadcasted_iota(jnp.int32, scores.shape, 1) & 255
            )
            scores = jnp.where(seen, scores, NEGATIVE)
        else:
            scores = jnp.concatenate(
                [
                    scores[i * HALF : (i + 1) * HALF] + jnp.where(o <= sp, 0.0, NEGATIVE).astype(F32)
                    for i, o in enumerate(blocks)
                ],
                axis=0,
            )
        old = peak[...]
        new = jnp.maximum(old, jnp.max(scores, axis=0, keepdims=True))
        shrink = jnp.exp2(old - new)
        wt = jnp.exp2(scores - new)
        peak[...] = new
        total[...] = total[...] * shrink + jnp.sum(wt, axis=0, keepdims=True)
        wt = wt.astype(BF16)
        accum[0:128, :] = accum[0:128, :] * shrink[:, 0:256] + jnp.dot(
            values[0:128], wt[:, 0:256], preferred_element_type=F32
        )
        accum[128:192, :] = accum[128:192, :] * shrink[:, 256:512] + jnp.dot(
            values[128:192], wt[:, 256:512], preferred_element_type=F32
        )

    def begin(halves, slot):
        keys, vals = project(halves)
        raw = jnp.dot(keys, qt[...], preferred_element_type=F32)
        score[slot] = raw
        value[slot] = vals
        for i in range(4):
            most[slot, i : i + 1, :] = jnp.max(raw[i * HALF : (i + 1) * HALF], axis=0, keepdims=True)

    def finish(blocks, there, slot):
        hidden = [jnp.where((o <= sp) & there, 0.0, NEGATIVE).astype(F32) for o in blocks]
        old = peak[...]
        new = old
        for i in range(4):
            new = jnp.maximum(new, most[slot, i : i + 1, :] * factor + hidden[i])
        shrink = jnp.exp2(old - new)
        peak[...] = new
        parts = [
            jnp.exp2(score[slot, i * HALF : (i + 1) * HALF, :] * factor - (new - hidden[i])) for i in range(4)
        ]
        total[...] = total[...] * shrink + jnp.sum(
            (parts[0] + parts[1]) + (parts[2] + parts[3]), axis=0, keepdims=True
        )
        wt = jnp.concatenate([p.astype(BF16) for p in parts], axis=0)
        accum[0:128, :] = accum[0:128, :] * shrink[:, 0:256] + jnp.dot(
            value[slot, 0:128, :], wt[:, 0:256], preferred_element_type=F32
        )
        accum[128:192, :] = accum[128:192, :] * shrink[:, 256:512] + jnp.dot(
            value[slot, 128:192, :], wt[:, 256:512], preferred_element_type=F32
        )

    peak[...] = jnp.full_like(peak, NEGATIVE)
    total[...] = jnp.zeros_like(total)
    accum[...] = jnp.zeros_like(accum)
    fold([pieces.at[0], pieces.at[1]], None)

    def given(n, count):
        ref = two if count == 2 else lat.at[0, 0]
        remote(ref, ref, p_send.at[0], p_recv.at[n], partner).wait_recv()

    def blocks_of(n):
        kp, km, d = ring_step(n)
        return (
            at(a + rel(kp), b - d), at(a + rel(km), b + d), turned(b + rel(kp), a - d), turned(b + rel(km), a + d)
        )

    def halves_of(o):
        return [lat.at[core, o[0]], lat.at[core, o[1]], lat.at[other, o[2]], lat.at[other, o[3]]]

    def least(o):
        return jnp.minimum(jnp.minimum(o[0], o[1]), jnp.minimum(o[2], o[3]))

    def near_blocks(n):
        return at(a + rel(n), b), turned(b + rel(n), a)

    latents.spread(jnp.int32(0), pieces.at[core])

    def near_pair(n, slot):
        given(n, 1)
        given(n + 1, 1)
        one, two_ = near_blocks(n), near_blocks(n + 1)
        o = (one[0], two_[0], one[1], two_[1])
        begin(halves_of(o), slot)
        return o

    one_, two__, three, four, five, six, seven = (jnp.int32(i) for i in range(1, 8))
    latent_near(one_)
    latent_near(two__)
    latent_near(three)
    latent_near(four)
    latents.spread(one_)
    latents.spread(two__)
    wown[...] = jnp.zeros_like(wown)
    wown[:, 0:352] = gate_w[...]
    wown[:, 384:736] = up_w[...]
    wown[:, 768:1120] = down_w[...]
    score[...] = jnp.zeros_like(score)
    value[...] = jnp.zeros_like(value)
    most[...] = jnp.zeros_like(most)
    finish(near_pair(one_, 0), sp >= 0, 0)
    latents.spread(three)
    latents.spread(four)
    latent_far(jnp.int32(8))
    finish(near_pair(three, 0), sp >= 0, 0)
    latent_near(five)
    latent_near(six)
    latent_near(seven)
    latents.spread(five)
    latents.spread(six)
    latents.spread(seven)
    latent_far(jnp.int32(9))
    latent_far(jnp.int32(10))
    last_near = near_pair(five, 1)
    given(jnp.int32(7), 1)
    seventh = near_blocks(jnp.int32(7))

    @pl.when(jnp.minimum(seventh[0], seventh[1]) <= sp)
    def _():
        fold([lat.at[core, seventh[0]], lat.at[other, seventh[1]]], seventh)

    @pl.loop(0, 14)
    def _(m):
        n = 8 + 2 * m

        @pl.when(n + 3 < 36)
        def _():
            latent_far(n + 3)

        @pl.when(n + 4 < 36)
        def _():
            latent_far(n + 4)

        @pl.when(m == 1)
        def _():
            weights.start()

        @pl.when((m == 4) | (m == 6) | (m == 8))
        def _():
            weights.near(m - 3)
            weights.near(m - 2)

        @pl.when(m == 10)
        def _():
            weights.near(m - 3)
            weights.spread(jnp.int32(0), wown)

            @pl.loop(1, 8)
            def _(k):
                weights.spread(k)

        @pl.when(m == 12)
        def _():
            weights.far(jnp.int32(8))

        @pl.when(m == 13)
        def _():
            weights.far(jnp.int32(9))
            weights.far(jnp.int32(10))

        @pl.when(m == 5)
        def _():
            share_rows()

        @pl.when(m == 9)
        def _():
            share_near()

        now, after = blocks_of(n), blocks_of(n + 1)
        past = blocks_of(n - 1)
        before = [jnp.where(m == 0, o, p) for o, p in zip(last_near, past)]
        given(n, 2)
        given(n + 1, 2)

        @pl.when(jnp.minimum(jnp.minimum(least(before), least(now)), least(after)) <= sp)
        def _():
            begin(halves_of(now), 0)
            finish(before, m >= 0, 1)
            begin(halves_of(after), 1)
            finish(now, m >= 0, 0)

    finish(blocks_of(jnp.int32(35)), sp >= 0, 1)

    result = accum[...]
    att[tp, 0:128, :] = (result[0:128] / total[:, 0:256]).astype(BF16)
    att[tp, 128:192, :] = (result[128:192] / total[:, 256:512]).astype(BF16)

    weights.far(jnp.int32(11))

    def att_copy(t, half, i, dev):
        ref = att.at[t] if half is None else att.at[t, half]
        return remote(ref, ref, a_send.at[i], a_recv.at[i], dev)

    for half, i, dev in ((top, 0, x_up), (low, 2, x_dn), (low, 1, x_up), (top, 3, x_dn), (None, 6, partner)):
        att_copy(tp, half, i, dev).start()

    share_far()

    @pl.loop(12, 15)
    def _(n):
        weights.far(n)

    t_up, t_dn, t_far = across(3), across(1), across(2)
    att_copy(t_up, top, 0, partner).wait_recv()
    att_copy(t_up, top, 4, x_up).start()
    att_copy(t_dn, low, 2, partner).wait_recv()
    att_copy(t_dn, low, 5, x_dn).start()
    weights.far(jnp.int32(15))
    att_copy(t_up, low, 1, partner).wait_recv()
    att_copy(t_up, None, 8, partner).start()
    att_copy(t_dn, top, 3, partner).wait_recv()
    att_copy(t_dn, None, 7, partner).start()

    @pl.loop(16, 18)
    def _(n):
        weights.far(n)

    att_copy(t_far, top, 4, partner).wait_recv()
    att_copy(t_far, top, 9, partner).start()
    att_copy(t_far, low, 5, partner).wait_recv()
    att_copy(t_far, low, 10, partner).start()
    weights.far(jnp.int32(18))

    for half, i in ((None, 6), (None, 7), (None, 8), (top, 9), (low, 10)):
        att_copy(tp, half, i, partner).wait_recv()

    for i in (0, 1, 2, 3):
        t = 2 * rem(xx + i, 4) + other
        remote(rows.at[t], rows.at[t], r_send.at[0], r_recv.at[t], partner).wait_recv()
        if i == 2:
            for j, rest in ((10, top), (11, low)):
                remote(wout.at[t, rest], wout.at[t, rest], o_send.at[0], o_recv.at[j], partner).wait_recv()
        else:
            remote(wout.at[t], wout.at[t], o_send.at[0], o_recv.at[t], partner).wait_recv()

    @pl.loop(0, 8)
    def _(t):
        att_t[t] = att[t].T

    @pl.loop(0, 4)
    def _(j):
        cols = pl.ds(pl.multiple_of(j * 512, 512), 512)
        acc = jnp.dot(att_t[0], wout[0, :, cols], preferred_element_type=F32)
        for t in range(1, 8):
            acc = acc + jnp.dot(att_t[t], wout[t, :, cols], preferred_element_type=F32)
        hs[:, cols] = acc
        weights.far(19 + 2 * j)
        weights.far(20 + 2 * j)

    for i in range(7):
        remote(rows.at[tp], rows.at[tp], r_send.at[i], r_recv.at[tp], partner).wait_send()

    @pl.loop(0, 8)
    def _(t):
        chunk = pl.ds(pl.multiple_of(t * 32, 32), 32)
        value = hs[chunk, :]
        scale = lax.rsqrt(jnp.mean(value * value, axis=-1, keepdims=True) + EPS)
        mixed = (rows[t].astype(F32) + value * scale * again[...]).astype(BF16)
        rows[t] = mixed
        value = mixed.astype(F32)
        scale = lax.rsqrt(jnp.mean(value * value, axis=-1, keepdims=True) + EPS)
        norm[chunk, :] = (value * scale * mgain[...]).astype(BF16)
        weights.far(27 + t)

    weights.far(jnp.int32(35))

    wts[sp] = wown[...]
    both = jnp.dot(norm[...], wts[:, :, 0:768].reshape(2048, 768), preferred_element_type=F32)
    gate, up = both[:, 0:384], both[:, 384:768]
    hid[...] = (gate / (1.0 + jnp.exp(-gate)) * up).astype(BF16)

    @pl.loop(0, 2)
    def _(j):
        down = wts[pl.ds(j * 32, 32), :, 768:1152].reshape(1024, 384)
        block = lax.dot_general(hid[...], down, (((1,), (1,)), ((), ())), preferred_element_type=F32)
        part[:, :, pl.ds(pl.multiple_of(j * 1024, 1024), 1024)] = block.astype(BF16).reshape(8, 32, 1024)

    for i in (2, 1, 3, 0):
        x_to = rem(xx + i, 4)
        remote(part.at[2 * x_to + other], pbuf.at[x_to], s_send.at[i], s_recv.at[i], partner).start()
    def chip_sum(i):
        x_to = rem(xx + i, 4)
        remote(pbuf.at[x_to], pbuf.at[x_to], s_send.at[i], s_recv.at[i], partner).wait_recv()
        return part[2 * x_to + core].astype(F32) + pbuf[x_to].astype(F32)

    upper, under = pl.ds(0, 16), pl.ds(16, 16)

    def along(src, dst, i, dev):
        return remote(src, dst, s_send.at[i], s_recv.at[i], dev)

    far_sum = chip_sum(2)
    sbuf[1] = far_sum.astype(BF16)
    up_sum = chip_sum(1)
    sbuf[0] = up_sum.astype(BF16)
    along(sbuf.at[1, upper], rbuf.at[1, upper], 4, x_up).start()
    along(sbuf.at[1, under], rbuf.at[1, under], 5, x_dn).start()
    dn_sum = chip_sum(3)
    sbuf[2] = dn_sum.astype(BF16)
    along(sbuf.at[0, under], rbuf.at[0, under], 6, x_up).start()
    summed = chip_sum(0)
    along(sbuf.at[2, upper], rbuf.at[2, upper], 7, x_dn).start()

    @pl.loop(0, 8)
    def _(n):
        for sems in (plus, minus):
            weights.free(sems.at[n])
        given_free(n, 2)

        @pl.when(n != 6)
        def _():
            weights.free(first.at[n])

    for i in range(11):
        half = (top, low, low, top, top, low, None, None, None, top, low)[i]
        att_copy(tp, half, i, partner).wait_send()
    for i in (0, 1, 2, 5, 6):
        remote(wout.at[tp], wout.at[tp], o_send.at[i], o_recv.at[tp], partner).wait_send()
    for i in (3, 4, 7, 8):
        remote(wout.at[tp, top], wout.at[tp, top], o_send.at[i], o_recv.at[tp], partner).wait_send()

    along(rbuf.at[1, upper], rbuf.at[1, upper], 4, partner).wait_recv()
    cbuf[0] = (sums_of(part, pbuf, rem(xx + 1, 4), core, 0) + rbuf[1, 0:16].astype(F32)).astype(BF16)
    along(rbuf.at[1, under], rbuf.at[1, under], 5, partner).wait_recv()
    cbuf[1] = (sums_of(part, pbuf, rem(xx + 3, 4), core, 16) + rbuf[1, 16:32].astype(F32)).astype(BF16)
    along(cbuf.at[0], rbuf.at[0, upper], 8, x_up).start()
    along(cbuf.at[1], rbuf.at[2, under], 9, x_dn).start()
    along(rbuf.at[0, under], rbuf.at[0, under], 6, partner).wait_recv()
    along(rbuf.at[2, upper], rbuf.at[2, upper], 7, partner).wait_recv()
    along(rbuf.at[0, upper], rbuf.at[0, upper], 8, partner).wait_recv()
    along(rbuf.at[2, under], rbuf.at[2, under], 9, partner).wait_recv()
    summed = summed + (rbuf[0].astype(F32) + rbuf[2].astype(F32))
    out[...] = (rows[tp].astype(F32) + 0.5 * summed).astype(BF16)

    for i in range(4):
        remote(rbuf.at[0], rbuf.at[0], s_send.at[i], s_recv.at[i], partner).wait_send()
    for i in range(4, 10):
        along(rbuf.at[0, upper], rbuf.at[0, upper], i, partner).wait_send()


def sums_of(part, pbuf, x_to, core, start):
    rows = slice(start, start + 16)
    return part[2 * x_to + core, rows].astype(F32) + pbuf[x_to, rows].astype(F32)


def shards(
    residual_in, query_lean, query_broad, latent, rope_key, latent_gain, key_up_lean, key_up_broad, value_up_lean,
    value_up_broad, out_lean, out_broad, attn_gain, mlp_gain, gate_weight, up_weight, down_weight,
):
    tokens = latent.shape[0]
    positions = lax.axis_index("sp") * tokens + jnp.arange(tokens, dtype=jnp.int32)
    freqs = THETA ** (-2.0 * jnp.arange(16, dtype=F32) / 32)
    angle = freqs[:, None] * positions.astype(F32)[None, :]
    vmem = pl.BlockSpec(memory_space=pltpu.VMEM)
    hbm = pl.BlockSpec(memory_space=pl.ANY)
    sems = pltpu.SemaphoreType.DMA
    loaded = [
        ((256, 256), BF16), ((1, 256), F32), ((32, 256), BF16), ((16, 256), F32), ((16, 256), F32), ((160, 256), BF16),
        ((96, 256), BF16), ((256, 128), BF16), ((64, 256), BF16), ((256, 128), BF16), ((64, 256), BF16),
        ((1, 2048), F32), ((1, 2048), F32), ((32, 352), BF16), ((32, 352), BF16), ((32, 352), BF16),
    ]
    scratch = [pltpu.VMEM(shape, dtype) for shape, dtype in loaded] + [
        pltpu.VMEM((2, PIECE, 256), BF16),
        pltpu.VMEM((2, 512, 512), F32),
        pltpu.VMEM((2, 192, 512), BF16),
        pltpu.VMEM((2, 8, 512), F32),
        pltpu.VMEM((2, 64, PIECE, 256), BF16),
        pltpu.VMEM((64, 32, 1152), BF16),
        pltpu.VMEM((8, 192, 2048), BF16),
        pltpu.VMEM((8, 32, 2048), BF16),
        pltpu.VMEM((8, 192, 256), BF16),
        pltpu.VMEM((256, 512), BF16),
        pltpu.VMEM((256, 256), BF16),
        pltpu.VMEM((192, 256), BF16),
        pltpu.VMEM((32, 256), BF16),
        pltpu.VMEM((1, 512), F32),
        pltpu.VMEM((1, 512), F32),
        pltpu.VMEM((192, 256), F32),
        pltpu.VMEM((8, 256, 192), BF16),
        pltpu.VMEM((256, 2048), F32),
        pltpu.VMEM((256, 2048), BF16),
        pltpu.VMEM((256, 384), BF16),
        pltpu.VMEM((8, 32, 2048), BF16),
        pltpu.VMEM((4, 32, 2048), BF16),
        pltpu.VMEM((3, 32, 2048), BF16),
        pltpu.VMEM((3, 32, 2048), BF16),
        pltpu.VMEM((2, 16, 2048), BF16),
        pltpu.VMEM((32, 1152), BF16),
        sems((36,)), sems((36,)), sems((36,)), sems((8,)), sems((8,)), sems((8,)), sems((8,)),
        sems((3,)), sems((9,)), sems((12,)), sems((7,)), sems((8,)), sems((11,)), sems((11,)), sems((10,)), sems((10,)),
        sems((16,)),
    ]
    return pl.pallas_call(
        kernel,
        out_shape=jax.ShapeDtypeStruct((32, 2048), BF16),
        in_specs=[hbm] * 19,
        out_specs=vmem,
        scratch_shapes=scratch,
        compiler_params=pltpu.CompilerParams(
            collective_id=0, has_side_effects=True, vmem_limit_bytes=44 * 1024 * 1024
        ),
    )(
        *[pltpu.with_memory_space_constraint(v, pltpu.HBM) for v in (latent, latent_gain[None], rope_key.T)],
        jnp.cos(angle),
        jnp.sin(angle),
        *[
            pltpu.with_memory_space_constraint(v, pltpu.HBM)
            for v in (
                query_broad[:, 0].T, query_lean[:, 0].T, key_up_broad[:, 0], key_up_lean[:, 0].T, value_up_broad[:, 0],
                value_up_lean[:, 0].T, attn_gain[None], mlp_gain[None], gate_weight, up_weight, down_weight.T,
                out_broad[0], out_lean[0], residual_in,
            )
        ],
    )


def solution(mesh):
    in_specs = (
        P(("sp", "tp"), None), P("sp", "tp", None), P("sp", "tp", None), P("sp", None), P("sp", None), P(),
        P(None, "tp", None), P(None, "tp", None), P(None, "tp", None), P(None, "tp", None),
        P("tp", None, None), P("tp", None, None), P(), P(), P("sp", "tp"), P("sp", "tp"), P("tp", "sp"),
    )
    return jax.shard_map(
        shards, mesh=mesh, in_specs=in_specs, out_specs=P(("sp", "tp"), None), check_vma=False
    )
```

```python
import jax
import jax.numpy as jnp
from jax import lax
from jax.experimental import pallas as pl
from jax.experimental.pallas import tpu as pltpu
from jax.sharding import PartitionSpec as P

MESH = pl.DeviceIdType.MESH
THETA = 10000.0
EPS = 1e-06
NEGATIVE = -1e30
LOG2E = 1.4426950408889634
RING = 8
F32 = jnp.float32
BF16 = jnp.bfloat16

HALF = 128
PIECE = HALF + 16


def rem(v, n):
    return lax.rem(v, jnp.int32(n))


def div(v, n):
    return lax.div(v, jnp.int32(n))


def kernel(
    *args,
):
    inputs, (ob, ol, resid, out), rest = args[:16], args[16:20], args[20:]
    held, rest, in_sem = rest[:16], rest[16:-1], rest[-1]
    run(inputs, held, in_sem, ob, ol, resid, out, *rest)


def run(
    inputs, held, in_sem, ob, ol, resid, out,
    pieces, score, value, most, lat, wts, wout, rows, att, qt, kup, vupt, spread, peak, total, accum, att_t, hs, norm, hid, part, pbuf, sbuf, rbuf, cbuf, wown,
    l_recv, w_recv, p_recv, first, plus, minus, p_send,
    loc, o_send, o_recv, r_send, r_recv, a_send, a_recv, s_send, s_recv,
):
    sp = lax.axis_index("sp")
    tp = lax.axis_index("tp")
    core = rem(tp, 2)
    xx = div(tp, 2)
    other = 1 - core
    sa = 1 + 7 * core
    sb = 8 - 7 * core
    a = rem(lax.div(sp, sa), RING)
    b = rem(lax.div(sp, sb), RING)

    def at(i, j):
        return rem(i + 16, RING) * sa + rem(j + 16, RING) * sb

    def turned(i, j):
        return rem(i + 16, RING) * sb + rem(j + 16, RING) * sa

    def rel(k):
        return div(k + 1, 2) * (1 - 2 * rem(k, 2))

    a_up, a_dn, b_up, b_dn = (
        (at(a + 1, b), tp), (at(a - 1, b), tp), (at(a, b + 1), tp), (at(a, b - 1), tp)
    )
    a_up2, a_dn2 = (at(a + 2, b), tp), (at(a - 2, b), tp)
    partner = (sp, 2 * xx + other)

    def across(step):
        return 2 * rem(xx + step, 4) + core

    x_up, x_far, x_dn = (sp, across(1)), (sp, across(2)), (sp, across(3))

    def remote(src, dst, ssem, rsem, dev):
        return pltpu.make_async_remote_copy(
            src_ref=src, dst_ref=dst, send_sem=ssem, recv_sem=rsem, device_id=dev, device_id_type=MESH
        )

    latent, lgain, rope, cosine, sine, qb, ql, kb, kl, vb, vl, again, mgain, gate_w, up_w, down_w = held
    barrier = pltpu.get_barrier_semaphore()
    for dev in (a_up, a_dn, b_up, b_dn, partner, x_up, x_far, x_dn, a_up2, a_dn2):
        pl.semaphore_signal(barrier, inc=1, device_id=dev, device_id_type=MESH)
    loads = [pltpu.make_async_copy(src, dst, in_sem.at[i]) for i, (src, dst) in enumerate(zip(inputs, held))]
    for load in loads:
        load.start()

    own_b = pltpu.make_async_copy(ob, wout.at[tp, pl.ds(0, 128)], loc.at[0])
    own_l = pltpu.make_async_copy(ol, wout.at[tp, pl.ds(128, 64)], loc.at[1])
    own_r = pltpu.make_async_copy(resid, rows.at[tp], loc.at[2])
    own_b.start()
    own_l.start()
    own_r.start()

    for load in loads[:7]:
        load.wait()

    def rotated(ref, start):
        low, high = ref[start : start + 16, :].astype(F32), ref[start + 16 : start + 32, :].astype(F32)
        co, si = cosine[...], sine[...]
        return (low * co - high * si).astype(BF16), (low * si + high * co).astype(BF16)

    wide = latent[...].astype(F32)
    wide = (wide * lax.rsqrt(jnp.mean(wide * wide, axis=-1, keepdims=True) + EPS) * lgain[...]).astype(BF16)
    low, high = rotated(rope, 0)
    for h in range(2):
        pieces[h, 0:HALF, :] = wide[h * HALF : (h + 1) * HALF]
        pieces[h, HALF:PIECE, 0:HALF] = low[:, h * HALF : (h + 1) * HALF]
        pieces[h, HALF:PIECE, HALF:256] = high[:, h * HALF : (h + 1) * HALF]
    qt[128:256, :] = jnp.zeros((128, 512), BF16)
    qt[0:128, 256:512] = jnp.zeros((128, 256), BF16)
    qt[0:128, 0:256] = qb[0:128, :]
    qt[128:192, 256:512] = ql[0:64, :]
    for ref, start, at_column in ((qb, 128, 0), (ql, 64, 256)):
        low, high = rotated(ref, start)
        qt[192:208, at_column : at_column + 256] = low
        qt[208:224, at_column : at_column + 256] = high

    for load in loads[7:]:
        load.wait()
    pl.semaphore_wait(barrier, 10)

    class Stream:
        def __init__(self, own, slot, pair, recv, fresh):
            self.own, self.slot, self.pair, self.recv, self.fresh = own, slot, pair, recv, fresh

        def go(self, src, o, ssem, n, dev):
            remote(src, self.slot(o), ssem, self.recv.at[n], dev).start()

        def free(self, sem, when=True):
            if when is True:
                remote(self.slot(0), self.slot(0), sem, self.recv.at[0], partner).wait_send()
            else:
                pl.when(when)(lambda: self.free(sem))

        def start(self):
            for index, n, dev in ((0, 1, a_up), (7, 2, a_dn)):
                if not self.fresh:
                    self.free(first.at[index])
                self.go(self.own, sp, first.at[index], n, dev)

        def spread(self, k, src=None):
            o = at(a + rel(k), b)
            src = self.slot(o) if src is None else src
            for sems, dev in ((plus, b_up), (minus, b_dn)):
                if not self.fresh:
                    self.free(sems.at[k])
                self.go(src, o, sems.at[k], k + 8, dev)

        def near(self, k):
            o = at(a + rel(k), b)
            remote(self.slot(o), self.slot(o), first.at[0], self.recv.at[k], partner).wait_recv()

            @pl.when((rem(k, 2) == 1) & (k < 7))
            def _():
                if not self.fresh:
                    self.free(first.at[k])
                self.go(self.slot(o), o, first.at[k], k + 2, a_up)

            @pl.when((rem(k, 2) == 0) & (k < 6))
            def _():
                if not self.fresh:
                    self.free(first.at[k])
                self.go(self.slot(o), o, first.at[k], k + 2, a_dn)

        def far(self, n):
            kp, km, d = ring_step(n)
            k = rem(n, 8)
            op, om = at(a + rel(kp), b - d), at(a + rel(km), b + d)
            remote(self.pair, self.pair, first.at[0], self.recv.at[n], partner).wait_recv()

            @pl.when(n < 28)
            def _():
                self.free(plus.at[k])
                self.go(self.slot(op), op, plus.at[k], n + 8, b_up)

            @pl.when((n < 24) | ((n >= 28) & (n < 32)))
            def _():
                self.free(minus.at[k])
                self.go(self.slot(om), om, minus.at[k], jnp.where(n < 24, n + 8, n + 4), b_dn)

            return k, op, om

    def give(n, o):
        remote(lat.at[core, o], lat.at[core, o], p_send.at[rem(n, 8)], p_recv.at[n], partner).start()

    two = lat.at[0, pl.ds(0, 2)]

    def given_free(n, count):
        ref = two if count == 2 else lat.at[0, 0]
        remote(ref, ref, p_send.at[rem(n, 8)], p_recv.at[0], partner).wait_send()

    def ring_step(n):
        last = div(n, 32)
        kp = rem(n, 8)
        return kp, kp + 4 * last, div(n, 8)

    latents = Stream(pieces.at[core], lambda o: lat.at[core, o], two, l_recv, True)
    weights = Stream(wown, lambda o: wts.at[o], wts.at[pl.ds(0, 2)], w_recv, False)

    def latent_near(k):
        o = at(a + rel(k), b)
        remote(lat.at[core, o], lat.at[core, o], first.at[0], l_recv.at[k], partner).wait_recv()

        @pl.when((k == 1) | (k == 3))
        def _():
            latents.go(lat.at[core, o], o, first.at[k], k + 4, a_up2)

        @pl.when(k == 2)
        def _():
            latents.go(lat.at[core, o], o, first.at[k], k + 4, a_dn2)

        give(k, o)

    def latent_far(n):
        k, op, om = latents.far(n)

        @pl.when(n >= 16)
        def _():
            given_free(n, 2)

        @pl.when((n > 8) & (n < 16))
        def _():
            given_free(n, 1)

        give(n, op)
        give(n, om)

    latents.start()
    latents.go(latents.own, sp, first.at[5], 3, a_up2)
    latents.go(latents.own, sp, first.at[4], 4, a_dn2)

    own_r.wait()
    for i, dev in enumerate((partner, x_up, x_dn, x_far)):
        remote(rows.at[tp], rows.at[tp], r_send.at[i], r_recv.at[tp], dev).start()
    own_b.wait()
    own_l.wait()
    for i, dev in enumerate((partner, x_up, x_dn)):
        remote(wout.at[tp], wout.at[tp], o_send.at[i], o_recv.at[tp], dev).start()

    def share_rows():
        for i in (1, 2, 3):
            t = across(i)
            remote(rows.at[t], rows.at[t], r_send.at[3 + i], r_recv.at[t], partner).wait_recv()
            remote(rows.at[t], rows.at[t], r_send.at[3 + i], r_recv.at[t], partner).start()

    top, low = pl.ds(0, 96), pl.ds(96, 96)

    def share_near():
        for i, t, rest, dev in ((3, across(3), top, x_up), (4, across(1), low, x_dn)):
            remote(wout.at[t], wout.at[t], o_send.at[i], o_recv.at[t], partner).wait_recv()
            far = 8 if i == 3 else 9
            remote(wout.at[t, rest], wout.at[t, rest], o_send.at[i], o_recv.at[far], dev).start()
            remote(wout.at[t], wout.at[t], o_send.at[i + 2], o_recv.at[t], partner).start()

    def share_far():
        t = across(2)
        for i, rest in ((8, top), (9, low)):
            remote(wout.at[t, rest], wout.at[t, rest], o_send.at[0], o_recv.at[i], partner).wait_recv()
            remote(wout.at[t, rest], wout.at[t, rest], o_send.at[i - 1], o_recv.at[i + 2], partner).start()

    kup[...] = jnp.zeros_like(kup)
    kup[:, 0:128] = kb[...]
    kup[:, 128:192] = kl[...].T
    vupt[0:128, :] = vb[...].T
    vupt[128:192, :] = vl[...]
    spread[...] = (
        lax.broadcasted_iota(jnp.int32, (32, 256), 1) == lax.broadcasted_iota(jnp.int32, (32, 256), 0) + 192
    ).astype(F32).astype(BF16)

    column = lax.broadcasted_iota(jnp.int32, (1, 512), 1)
    factor = jnp.where(column < 256, LOG2E * 160 ** (-0.5), LOG2E * 96 ** (-0.5)).astype(F32)

    def project(halves):
        rows_of = jnp.concatenate([h[0:HALF, :] for h in halves], axis=0)
        turned_rot = jnp.concatenate(
            [
                jnp.concatenate([h[HALF:PIECE, 0:HALF] for h in halves], axis=1),
                jnp.concatenate([h[HALF:PIECE, HALF:256] for h in halves], axis=1),
            ],
            axis=0,
        )
        keys = jnp.dot(rows_of, kup[...], preferred_element_type=F32) + lax.dot_general(
            turned_rot, spread[...], (((0,), (0,)), ((), ())), preferred_element_type=F32
        )
        values = lax.dot_general(
            vupt[...], rows_of, (((1,), (1,)), ((), ())), preferred_element_type=F32
        )
        return keys.astype(BF16), values.astype(BF16)

    def fold(halves, blocks):
        keys, values = project(halves)
        scores = jnp.dot(keys, qt[...], preferred_element_type=F32) * factor
        if blocks is None:
            seen = lax.broadcasted_iota(jnp.int32, scores.shape, 0) <= (
                lax.broadcasted_iota(jnp.int32, scores.shape, 1) & 255
            )
            scores = jnp.where(seen, scores, NEGATIVE)
        else:
            scores = jnp.concatenate(
                [
                    scores[i * HALF : (i + 1) * HALF] + jnp.where(o <= sp, 0.0, NEGATIVE).astype(F32)
                    for i, o in enumerate(blocks)
                ],
                axis=0,
            )
        old = peak[...]
        new = jnp.maximum(old, jnp.max(scores, axis=0, keepdims=True))
        shrink = jnp.exp2(old - new)
        wt = jnp.exp2(scores - new)
        peak[...] = new
        total[...] = total[...] * shrink + jnp.sum(wt, axis=0, keepdims=True)
        wt = wt.astype(BF16)
        accum[0:128, :] = accum[0:128, :] * shrink[:, 0:256] + jnp.dot(
            values[0:128], wt[:, 0:256], preferred_element_type=F32
        )
        accum[128:192, :] = accum[128:192, :] * shrink[:, 256:512] + jnp.dot(
            values[128:192], wt[:, 256:512], preferred_element_type=F32
        )

    def begin(halves, slot):
        keys, vals = project(halves)
        raw = jnp.dot(keys, qt[...], preferred_element_type=F32)
        score[slot] = raw
        value[slot] = vals
        for i in range(4):
            most[slot, i : i + 1, :] = jnp.max(raw[i * HALF : (i + 1) * HALF], axis=0, keepdims=True)

    def finish(blocks, there, slot):
        hidden = [jnp.where((o <= sp) & there, 0.0, NEGATIVE).astype(F32) for o in blocks]
        old = peak[...]
        new = old
        for i in range(4):
            new = jnp.maximum(new, most[slot, i : i + 1, :] * factor + hidden[i])
        shrink = jnp.exp2(old - new)
        peak[...] = new
        parts = [
            jnp.exp2(score[slot, i * HALF : (i + 1) * HALF, :] * factor - (new - hidden[i])) for i in range(4)
        ]
        total[...] = total[...] * shrink + jnp.sum(
            (parts[0] + parts[1]) + (parts[2] + parts[3]), axis=0, keepdims=True
        )
        wt = jnp.concatenate([p.astype(BF16) for p in parts], axis=0)
        accum[0:128, :] = accum[0:128, :] * shrink[:, 0:256] + jnp.dot(
            value[slot, 0:128, :], wt[:, 0:256], preferred_element_type=F32
        )
        accum[128:192, :] = accum[128:192, :] * shrink[:, 256:512] + jnp.dot(
            value[slot, 128:192, :], wt[:, 256:512], preferred_element_type=F32
        )

    peak[...] = jnp.full_like(peak, NEGATIVE)
    total[...] = jnp.zeros_like(total)
    accum[...] = jnp.zeros_like(accum)
    fold([pieces.at[0], pieces.at[1]], None)

    def given(n, count):
        ref = two if count == 2 else lat.at[0, 0]
        remote(ref, ref, p_send.at[0], p_recv.at[n], partner).wait_recv()

    def blocks_of(n):
        kp, km, d = ring_step(n)
        return (
            at(a + rel(kp), b - d), at(a + rel(km), b + d), turned(b + rel(kp), a - d), turned(b + rel(km), a + d)
        )

    def halves_of(o):
        return [lat.at[core, o[0]], lat.at[core, o[1]], lat.at[other, o[2]], lat.at[other, o[3]]]

    def least(o):
        return jnp.minimum(jnp.minimum(o[0], o[1]), jnp.minimum(o[2], o[3]))

    def near_blocks(n):
        return at(a + rel(n), b), turned(b + rel(n), a)

    latents.spread(jnp.int32(0), pieces.at[core])

    def near_pair(n, slot):
        given(n, 1)
        given(n + 1, 1)
        one, two_ = near_blocks(n), near_blocks(n + 1)
        o = (one[0], two_[0], one[1], two_[1])
        begin(halves_of(o), slot)
        return o

    one_, two__, three, four, five, six, seven = (jnp.int32(i) for i in range(1, 8))
    latent_near(one_)
    latent_near(two__)
    latent_near(three)
    latent_near(four)
    latents.spread(one_)
    latents.spread(two__)
    wown[...] = jnp.zeros_like(wown)
    wown[:, 0:352] = gate_w[...]
    wown[:, 384:736] = up_w[...]
    wown[:, 768:1120] = down_w[...]
    score[...] = jnp.zeros_like(score)
    value[...] = jnp.zeros_like(value)
    most[...] = jnp.zeros_like(most)
    finish(near_pair(one_, 0), sp >= 0, 0)
    latents.spread(three)
    latents.spread(four)
    latent_far(jnp.int32(8))
    finish(near_pair(three, 0), sp >= 0, 0)
    latent_near(five)
    latent_near(six)
    latent_near(seven)
    latents.spread(five)
    latents.spread(six)
    latents.spread(seven)
    latent_far(jnp.int32(9))
    latent_far(jnp.int32(10))
    last_near = near_pair(five, 1)
    given(jnp.int32(7), 1)
    seventh = near_blocks(jnp.int32(7))

    @pl.when(jnp.minimum(seventh[0], seventh[1]) <= sp)
    def _():
        fold([lat.at[core, seventh[0]], lat.at[other, seventh[1]]], seventh)

    @pl.loop(0, 14)
    def _(m):
        n = 8 + 2 * m

        @pl.when(n + 3 < 36)
        def _():
            latent_far(n + 3)

        @pl.when(n + 4 < 36)
        def _():
            latent_far(n + 4)

        @pl.when(m == 1)
        def _():
            weights.start()

        @pl.when((m == 4) | (m == 6) | (m == 8))
        def _():
            weights.near(m - 3)
            weights.near(m - 2)

        @pl.when(m == 10)
        def _():
            weights.near(m - 3)
            weights.spread(jnp.int32(0), wown)

            @pl.loop(1, 8)
            def _(k):
                weights.spread(k)

        @pl.when(m == 12)
        def _():
            weights.far(jnp.int32(8))

        @pl.when(m == 13)
        def _():
            weights.far(jnp.int32(9))
            weights.far(jnp.int32(10))

        @pl.when(m == 5)
        def _():
            share_rows()

        @pl.when(m == 9)
        def _():
            share_near()

        now, after = blocks_of(n), blocks_of(n + 1)
        past = blocks_of(n - 1)
        before = [jnp.where(m == 0, o, p) for o, p in zip(last_near, past)]
        given(n, 2)
        given(n + 1, 2)

        @pl.when(jnp.minimum(jnp.minimum(least(before), least(now)), least(after)) <= sp)
        def _():
            begin(halves_of(now), 0)
            finish(before, m >= 0, 1)
            begin(halves_of(after), 1)
            finish(now, m >= 0, 0)

    finish(blocks_of(jnp.int32(35)), sp >= 0, 1)

    result = accum[...]
    att[tp, 0:128, :] = (result[0:128] / total[:, 0:256]).astype(BF16)
    att[tp, 128:192, :] = (result[128:192] / total[:, 256:512]).astype(BF16)

    share_far()

    def att_copy(t, half, i, dev):
        ref = att.at[t] if half is None else att.at[t, half]
        return remote(ref, ref, a_send.at[i], a_recv.at[i], dev)

    for half, i, dev in ((top, 0, x_up), (low, 2, x_dn), (low, 1, x_up), (top, 3, x_dn), (None, 6, partner)):
        att_copy(tp, half, i, dev).start()

    @pl.loop(11, 17)
    def _(n):
        weights.far(n)

    t_up, t_dn, t_far = across(3), across(1), across(2)
    att_copy(t_up, top, 0, partner).wait_recv()
    att_copy(t_up, top, 4, x_up).start()
    att_copy(t_dn, low, 2, partner).wait_recv()
    att_copy(t_dn, low, 5, x_dn).start()
    weights.far(jnp.int32(17))
    weights.far(jnp.int32(18))
    att_copy(t_up, low, 1, partner).wait_recv()
    att_copy(t_up, None, 8, partner).start()
    att_copy(t_dn, top, 3, partner).wait_recv()
    att_copy(t_dn, None, 7, partner).start()

    @pl.loop(19, 21)
    def _(n):
        weights.far(n)

    att_copy(t_far, top, 4, partner).wait_recv()
    att_copy(t_far, top, 9, partner).start()
    att_copy(t_far, low, 5, partner).wait_recv()
    att_copy(t_far, low, 10, partner).start()
    weights.far(jnp.int32(21))
    weights.far(jnp.int32(22))

    for half, i in ((None, 6), (None, 7), (None, 8), (top, 9), (low, 10)):
        att_copy(tp, half, i, partner).wait_recv()

    for i in (0, 1, 2, 3):
        t = 2 * rem(xx + i, 4) + other
        remote(rows.at[t], rows.at[t], r_send.at[0], r_recv.at[t], partner).wait_recv()
        if i == 2:
            for j, rest in ((10, top), (11, low)):
                remote(wout.at[t, rest], wout.at[t, rest], o_send.at[0], o_recv.at[j], partner).wait_recv()
        else:
            remote(wout.at[t], wout.at[t], o_send.at[0], o_recv.at[t], partner).wait_recv()

    @pl.loop(0, 8)
    def _(t):
        att_t[t] = att[t].T

    @pl.loop(0, 4)
    def _(j):
        cols = pl.ds(pl.multiple_of(j * 512, 512), 512)
        acc = jnp.dot(att_t[0], wout[0, :, cols], preferred_element_type=F32)
        for t in range(1, 8):
            acc = acc + jnp.dot(att_t[t], wout[t, :, cols], preferred_element_type=F32)
        hs[:, cols] = acc
        weights.far(23 + 2 * j)
        weights.far(24 + 2 * j)

    for i in range(7):
        remote(rows.at[tp], rows.at[tp], r_send.at[i], r_recv.at[tp], partner).wait_send()

    @pl.loop(0, 8)
    def _(t):
        chunk = pl.ds(pl.multiple_of(t * 32, 32), 32)
        value = hs[chunk, :]
        scale = lax.rsqrt(jnp.mean(value * value, axis=-1, keepdims=True) + EPS)
        mixed = (rows[t].astype(F32) + value * scale * again[...]).astype(BF16)
        rows[t] = mixed
        value = mixed.astype(F32)
        scale = lax.rsqrt(jnp.mean(value * value, axis=-1, keepdims=True) + EPS)
        norm[chunk, :] = (value * scale * mgain[...]).astype(BF16)

        @pl.when(t < 5)
        def _():
            weights.far(31 + t)


    wts[sp] = wown[...]
    both = jnp.dot(norm[...], wts[:, :, 0:768].reshape(2048, 768), preferred_element_type=F32)
    gate, up = both[:, 0:384], both[:, 384:768]
    hid[...] = (gate / (1.0 + jnp.exp(-gate)) * up).astype(BF16)

    upper, under = pl.ds(0, 16), pl.ds(16, 16)
    sides = (pl.ds(0, 1024), pl.ds(1024, 1024))

    def chip_copy(i, q):
        x_to = rem(xx + i, 4)
        return remote(
            part.at[2 * x_to + other, :, sides[q]], pbuf.at[x_to, :, sides[q]], s_send.at[10 * q + i],
            s_recv.at[10 * q + i], partner,
        )

    def chip_sum(i, q):
        chip_copy(i, q).wait_recv()
        return both_of(i, q, slice(0, 32))

    def both_of(i, q, picked):
        x_to = rem(xx + i, 4)
        return part[2 * x_to + core, picked, sides[q]].astype(F32) + pbuf[x_to, picked, sides[q]].astype(F32)

    def along(src, dst, i, q, dev):
        return remote(src, dst, s_send.at[10 * q + i], s_recv.at[10 * q + i], dev)

    for q in range(2):
        down = wts[32 * q : 32 * q + 32, :, 768:1152].reshape(1024, 384)
        block = lax.dot_general(hid[...], down, (((1,), (1,)), ((), ())), preferred_element_type=F32)
        part[:, :, sides[q]] = block.astype(BF16).reshape(8, 32, 1024)
        for i in (2, 1, 3, 0):
            chip_copy(i, q).start()

    summed = []
    for q in range(2):
        side = sides[q]
        sbuf[1, :, side] = chip_sum(2, q).astype(BF16)
        sbuf[0, :, side] = chip_sum(1, q).astype(BF16)
        along(sbuf.at[1, upper, side], rbuf.at[1, upper, side], 4, q, x_up).start()
        along(sbuf.at[1, under, side], rbuf.at[1, under, side], 5, q, x_dn).start()
        sbuf[2, :, side] = chip_sum(3, q).astype(BF16)
        along(sbuf.at[0, under, side], rbuf.at[0, under, side], 6, q, x_up).start()
        summed.append(chip_sum(0, q))
        along(sbuf.at[2, upper, side], rbuf.at[2, upper, side], 7, q, x_dn).start()

    @pl.loop(0, 8)
    def _(n):
        for sems in (plus, minus):
            weights.free(sems.at[n])
        given_free(n, 2)

        @pl.when(n != 6)
        def _():
            weights.free(first.at[n])

    for i in range(11):
        half = (top, low, low, top, top, low, None, None, None, top, low)[i]
        att_copy(tp, half, i, partner).wait_send()
    for i in (0, 1, 2, 5, 6):
        remote(wout.at[tp], wout.at[tp], o_send.at[i], o_recv.at[tp], partner).wait_send()
    for i in (3, 4, 7, 8):
        remote(wout.at[tp, top], wout.at[tp, top], o_send.at[i], o_recv.at[tp], partner).wait_send()

    for q in range(2):
        side = sides[q]
        along(rbuf.at[1, upper, side], rbuf.at[1, upper, side], 4, q, partner).wait_recv()
        cbuf[0, :, side] = (both_of(1, q, slice(0, 16)) + rbuf[1, 0:16, side].astype(F32)).astype(BF16)
        along(rbuf.at[1, under, side], rbuf.at[1, under, side], 5, q, partner).wait_recv()
        cbuf[1, :, side] = (both_of(3, q, slice(16, 32)) + rbuf[1, 16:32, side].astype(F32)).astype(BF16)
        along(cbuf.at[0, :, side], rbuf.at[0, upper, side], 8, q, x_up).start()
        along(cbuf.at[1, :, side], rbuf.at[2, under, side], 9, q, x_dn).start()
    for q in range(2):
        side = sides[q]
        for i, r, picked in ((6, 0, under), (7, 2, upper), (8, 0, upper), (9, 2, under)):
            along(rbuf.at[r, picked, side], rbuf.at[r, picked, side], i, q, partner).wait_recv()
        value_q = summed[q] + (rbuf[0, :, side].astype(F32) + rbuf[2, :, side].astype(F32))
        out[:, side] = (rows[tp, :, side].astype(F32) + 0.5 * value_q).astype(BF16)

    for q in range(2):
        for i in range(4):
            chip_copy(i, q).wait_send()
        for i in range(4, 10):
            along(rbuf.at[0, upper, sides[q]], rbuf.at[0, upper, sides[q]], i, q, partner).wait_send()


def shards(
    residual_in, query_lean, query_broad, latent, rope_key, latent_gain, key_up_lean, key_up_broad, value_up_lean,
    value_up_broad, out_lean, out_broad, attn_gain, mlp_gain, gate_weight, up_weight, down_weight,
):
    tokens = latent.shape[0]
    positions = lax.axis_index("sp") * tokens + jnp.arange(tokens, dtype=jnp.int32)
    freqs = THETA ** (-2.0 * jnp.arange(16, dtype=F32) / 32)
    angle = freqs[:, None] * positions.astype(F32)[None, :]
    vmem = pl.BlockSpec(memory_space=pltpu.VMEM)
    hbm = pl.BlockSpec(memory_space=pl.ANY)
    sems = pltpu.SemaphoreType.DMA
    loaded = [
        ((256, 256), BF16), ((1, 256), F32), ((32, 256), BF16), ((16, 256), F32), ((16, 256), F32), ((160, 256), BF16),
        ((96, 256), BF16), ((256, 128), BF16), ((64, 256), BF16), ((256, 128), BF16), ((64, 256), BF16),
        ((1, 2048), F32), ((1, 2048), F32), ((32, 352), BF16), ((32, 352), BF16), ((32, 352), BF16),
    ]
    scratch = [pltpu.VMEM(shape, dtype) for shape, dtype in loaded] + [
        pltpu.VMEM((2, PIECE, 256), BF16),
        pltpu.VMEM((2, 512, 512), F32),
        pltpu.VMEM((2, 192, 512), BF16),
        pltpu.VMEM((2, 8, 512), F32),
        pltpu.VMEM((2, 64, PIECE, 256), BF16),
        pltpu.VMEM((64, 32, 1152), BF16),
        pltpu.VMEM((8, 192, 2048), BF16),
        pltpu.VMEM((8, 32, 2048), BF16),
        pltpu.VMEM((8, 192, 256), BF16),
        pltpu.VMEM((256, 512), BF16),
        pltpu.VMEM((256, 256), BF16),
        pltpu.VMEM((192, 256), BF16),
        pltpu.VMEM((32, 256), BF16),
        pltpu.VMEM((1, 512), F32),
        pltpu.VMEM((1, 512), F32),
        pltpu.VMEM((192, 256), F32),
        pltpu.VMEM((8, 256, 192), BF16),
        pltpu.VMEM((256, 2048), F32),
        pltpu.VMEM((256, 2048), BF16),
        pltpu.VMEM((256, 384), BF16),
        pltpu.VMEM((8, 32, 2048), BF16),
        pltpu.VMEM((4, 32, 2048), BF16),
        pltpu.VMEM((3, 32, 2048), BF16),
        pltpu.VMEM((3, 32, 2048), BF16),
        pltpu.VMEM((2, 16, 2048), BF16),
        pltpu.VMEM((32, 1152), BF16),
        sems((36,)), sems((36,)), sems((36,)), sems((8,)), sems((8,)), sems((8,)), sems((8,)),
        sems((3,)), sems((9,)), sems((12,)), sems((7,)), sems((8,)), sems((11,)), sems((11,)), sems((20,)), sems((20,)),
        sems((16,)),
    ]
    return pl.pallas_call(
        kernel,
        out_shape=jax.ShapeDtypeStruct((32, 2048), BF16),
        in_specs=[hbm] * 19,
        out_specs=vmem,
        scratch_shapes=scratch,
        compiler_params=pltpu.CompilerParams(
            collective_id=0, has_side_effects=True, vmem_limit_bytes=44 * 1024 * 1024
        ),
    )(
        *[pltpu.with_memory_space_constraint(v, pltpu.HBM) for v in (latent, latent_gain[None], rope_key.T)],
        jnp.cos(angle),
        jnp.sin(angle),
        *[
            pltpu.with_memory_space_constraint(v, pltpu.HBM)
            for v in (
                query_broad[:, 0].T, query_lean[:, 0].T, key_up_broad[:, 0], key_up_lean[:, 0].T, value_up_broad[:, 0],
                value_up_lean[:, 0].T, attn_gain[None], mlp_gain[None], gate_weight, up_weight, down_weight.T,
                out_broad[0], out_lean[0], residual_in,
            )
        ],
    )


def solution(mesh):
    in_specs = (
        P(("sp", "tp"), None), P("sp", "tp", None), P("sp", "tp", None), P("sp", None), P("sp", None), P(),
        P(None, "tp", None), P(None, "tp", None), P(None, "tp", None), P(None, "tp", None),
        P("tp", None, None), P("tp", None, None), P(), P(), P("sp", "tp"), P("sp", "tp"), P("tp", "sp"),
    )
    return jax.shard_map(
        shards, mesh=mesh, in_specs=in_specs, out_specs=P(("sp", "tp"), None), check_vma=False
    )
```

```python
import jax
import jax.numpy as jnp
from jax import lax
from jax.experimental import pallas as pl
from jax.experimental.pallas import tpu as pltpu
from jax.sharding import PartitionSpec as P

MESH = pl.DeviceIdType.MESH
THETA = 10000.0
EPS = 1e-06
NEGATIVE = -1e30
LOG2E = 1.4426950408889634
RING = 8
F32 = jnp.float32
BF16 = jnp.bfloat16

HALF = 128
PIECE = HALF + 16


def rem(v, n):
    return lax.rem(v, jnp.int32(n))


def div(v, n):
    return lax.div(v, jnp.int32(n))


def kernel(
    *args,
):
    inputs, (ob, ol, resid, out), rest = args[:16], args[16:20], args[20:]
    held, rest, in_sem = rest[:16], rest[16:-1], rest[-1]
    run(inputs, held, in_sem, ob, ol, resid, out, *rest)


def run(
    inputs, held, in_sem, ob, ol, resid, out,
    pieces, score, value, most, lat, wts, wout, rows, att, qt, kup, vupt, spread, peak, total, accum, att_t, hs, norm, hid, part, pbuf, sbuf, rbuf, cbuf, wown,
    l_recv, w_recv, p_recv, first, plus, minus, p_send,
    loc, o_send, o_recv, r_send, r_recv, a_send, a_recv, s_send, s_recv,
):
    sp = lax.axis_index("sp")
    tp = lax.axis_index("tp")
    core = rem(tp, 2)
    xx = div(tp, 2)
    other = 1 - core
    sa = 1 + 7 * core
    sb = 8 - 7 * core
    a = rem(lax.div(sp, sa), RING)
    b = rem(lax.div(sp, sb), RING)

    def at(i, j):
        return rem(i + 16, RING) * sa + rem(j + 16, RING) * sb

    def turned(i, j):
        return rem(i + 16, RING) * sb + rem(j + 16, RING) * sa

    def rel(k):
        return div(k + 1, 2) * (1 - 2 * rem(k, 2))

    a_up, a_dn, b_up, b_dn = (
        (at(a + 1, b), tp), (at(a - 1, b), tp), (at(a, b + 1), tp), (at(a, b - 1), tp)
    )
    a_up2, a_dn2 = (at(a + 2, b), tp), (at(a - 2, b), tp)
    partner = (sp, 2 * xx + other)

    def across(step):
        return 2 * rem(xx + step, 4) + core

    x_up, x_far, x_dn = (sp, across(1)), (sp, across(2)), (sp, across(3))

    def remote(src, dst, ssem, rsem, dev):
        return pltpu.make_async_remote_copy(
            src_ref=src, dst_ref=dst, send_sem=ssem, recv_sem=rsem, device_id=dev, device_id_type=MESH
        )

    latent, lgain, rope, cosine, sine, qb, ql, kb, kl, vb, vl, again, mgain, gate_w, up_w, down_w = held
    barrier = pltpu.get_barrier_semaphore()
    for dev in (a_up, a_dn, b_up, b_dn, partner, x_up, x_far, x_dn, a_up2, a_dn2):
        pl.semaphore_signal(barrier, inc=1, device_id=dev, device_id_type=MESH)
    loads = [pltpu.make_async_copy(src, dst, in_sem.at[i]) for i, (src, dst) in enumerate(zip(inputs, held))]
    for load in loads:
        load.start()

    own_b = pltpu.make_async_copy(ob, wout.at[tp, pl.ds(0, 128)], loc.at[0])
    own_l = pltpu.make_async_copy(ol, wout.at[tp, pl.ds(128, 64)], loc.at[1])
    own_r = pltpu.make_async_copy(resid, rows.at[tp], loc.at[2])
    own_b.start()
    own_l.start()
    own_r.start()

    for load in loads[:7]:
        load.wait()

    def rotated(ref, start):
        low, high = ref[start : start + 16, :].astype(F32), ref[start + 16 : start + 32, :].astype(F32)
        co, si = cosine[...], sine[...]
        return (low * co - high * si).astype(BF16), (low * si + high * co).astype(BF16)

    wide = latent[...].astype(F32)
    wide = (wide * lax.rsqrt(jnp.mean(wide * wide, axis=-1, keepdims=True) + EPS) * lgain[...]).astype(BF16)
    low, high = rotated(rope, 0)
    for h in range(2):
        pieces[h, 0:HALF, :] = wide[h * HALF : (h + 1) * HALF]
        pieces[h, HALF:PIECE, 0:HALF] = low[:, h * HALF : (h + 1) * HALF]
        pieces[h, HALF:PIECE, HALF:256] = high[:, h * HALF : (h + 1) * HALF]
    qt[128:256, :] = jnp.zeros((128, 512), BF16)
    qt[0:128, 256:512] = jnp.zeros((128, 256), BF16)
    qt[0:128, 0:256] = qb[0:128, :]
    qt[128:192, 256:512] = ql[0:64, :]
    for ref, start, at_column in ((qb, 128, 0), (ql, 64, 256)):
        low, high = rotated(ref, start)
        qt[192:208, at_column : at_column + 256] = low
        qt[208:224, at_column : at_column + 256] = high

    for load in loads[7:]:
        load.wait()
    pl.semaphore_wait(barrier, 10)

    class Stream:
        def __init__(self, own, slot, pair, recv, fresh):
            self.own, self.slot, self.pair, self.recv, self.fresh = own, slot, pair, recv, fresh

        def go(self, src, o, ssem, n, dev):
            remote(src, self.slot(o), ssem, self.recv.at[n], dev).start()

        def free(self, sem, when=True):
            if when is True:
                remote(self.slot(0), self.slot(0), sem, self.recv.at[0], partner).wait_send()
            else:
                pl.when(when)(lambda: self.free(sem))

        def start(self):
            for index, n, dev in ((0, 1, a_up), (7, 2, a_dn)):
                if not self.fresh:
                    self.free(first.at[index])
                self.go(self.own, sp, first.at[index], n, dev)

        def spread(self, k, src=None):
            o = at(a + rel(k), b)
            src = self.slot(o) if src is None else src
            for sems, dev in ((plus, b_up), (minus, b_dn)):
                if not self.fresh:
                    self.free(sems.at[k])
                self.go(src, o, sems.at[k], k + 8, dev)

        def near(self, k):
            o = at(a + rel(k), b)
            remote(self.slot(o), self.slot(o), first.at[0], self.recv.at[k], partner).wait_recv()

            @pl.when((rem(k, 2) == 1) & (k < 7))
            def _():
                if not self.fresh:
                    self.free(first.at[k])
                self.go(self.slot(o), o, first.at[k], k + 2, a_up)

            @pl.when((rem(k, 2) == 0) & (k < 6))
            def _():
                if not self.fresh:
                    self.free(first.at[k])
                self.go(self.slot(o), o, first.at[k], k + 2, a_dn)

        def far(self, n):
            kp, km, d = ring_step(n)
            k = rem(n, 8)
            op, om = at(a + rel(kp), b - d), at(a + rel(km), b + d)
            remote(self.pair, self.pair, first.at[0], self.recv.at[n], partner).wait_recv()

            @pl.when(n < 28)
            def _():
                self.free(plus.at[k])
                self.go(self.slot(op), op, plus.at[k], n + 8, b_up)

            @pl.when((n < 24) | ((n >= 28) & (n < 32)))
            def _():
                self.free(minus.at[k])
                self.go(self.slot(om), om, minus.at[k], jnp.where(n < 24, n + 8, n + 4), b_dn)

            return k, op, om

    def give(n, o):
        remote(lat.at[core, o], lat.at[core, o], p_send.at[rem(n, 8)], p_recv.at[n], partner).start()

    two = lat.at[0, pl.ds(0, 2)]

    def given_free(n, count):
        ref = two if count == 2 else lat.at[0, 0]
        remote(ref, ref, p_send.at[rem(n, 8)], p_recv.at[0], partner).wait_send()

    def ring_step(n):
        last = div(n, 32)
        kp = rem(n, 8)
        return kp, kp + 4 * last, div(n, 8)

    latents = Stream(pieces.at[core], lambda o: lat.at[core, o], two, l_recv, True)
    weights = Stream(wown, lambda o: wts.at[o], wts.at[pl.ds(0, 2)], w_recv, False)

    def latent_near(k):
        o = at(a + rel(k), b)
        remote(lat.at[core, o], lat.at[core, o], first.at[0], l_recv.at[k], partner).wait_recv()

        @pl.when((k == 1) | (k == 3))
        def _():
            latents.go(lat.at[core, o], o, first.at[k], k + 4, a_up2)

        @pl.when(k == 2)
        def _():
            latents.go(lat.at[core, o], o, first.at[k], k + 4, a_dn2)

        give(k, o)

    def latent_far(n):
        k, op, om = latents.far(n)

        @pl.when(n >= 16)
        def _():
            given_free(n, 2)

        @pl.when((n > 8) & (n < 16))
        def _():
            given_free(n, 1)

        give(n, op)
        give(n, om)

    latents.start()
    latents.go(latents.own, sp, first.at[5], 3, a_up2)
    latents.go(latents.own, sp, first.at[4], 4, a_dn2)

    own_r.wait()
    for i, dev in enumerate((partner, x_up, x_dn, x_far)):
        remote(rows.at[tp], rows.at[tp], r_send.at[i], r_recv.at[tp], dev).start()
    own_b.wait()
    own_l.wait()
    for i, dev in enumerate((partner, x_up, x_dn)):
        remote(wout.at[tp], wout.at[tp], o_send.at[i], o_recv.at[tp], dev).start()

    def share_rows():
        for i in (1, 2, 3):
            t = across(i)
            remote(rows.at[t], rows.at[t], r_send.at[3 + i], r_recv.at[t], partner).wait_recv()
            remote(rows.at[t], rows.at[t], r_send.at[3 + i], r_recv.at[t], partner).start()

    top, low = pl.ds(0, 96), pl.ds(96, 96)

    def share_near():
        for i, t, rest, dev in ((3, across(3), top, x_up), (4, across(1), low, x_dn)):
            remote(wout.at[t], wout.at[t], o_send.at[i], o_recv.at[t], partner).wait_recv()
            far = 8 if i == 3 else 9
            remote(wout.at[t, rest], wout.at[t, rest], o_send.at[i], o_recv.at[far], dev).start()
            remote(wout.at[t], wout.at[t], o_send.at[i + 2], o_recv.at[t], partner).start()

    def share_far():
        t = across(2)
        for i, rest in ((8, top), (9, low)):
            remote(wout.at[t, rest], wout.at[t, rest], o_send.at[0], o_recv.at[i], partner).wait_recv()
            remote(wout.at[t, rest], wout.at[t, rest], o_send.at[i - 1], o_recv.at[i + 2], partner).start()

    kup[...] = jnp.zeros_like(kup)
    kup[:, 0:128] = kb[...]
    kup[:, 128:192] = kl[...].T
    vupt[0:128, :] = vb[...].T
    vupt[128:192, :] = vl[...]
    spread[...] = (
        lax.broadcasted_iota(jnp.int32, (32, 256), 1) == lax.broadcasted_iota(jnp.int32, (32, 256), 0) + 192
    ).astype(F32).astype(BF16)

    column = lax.broadcasted_iota(jnp.int32, (1, 512), 1)
    factor = jnp.where(column < 256, LOG2E * 160 ** (-0.5), LOG2E * 96 ** (-0.5)).astype(F32)

    def project(halves):
        rows_of = jnp.concatenate([h[0:HALF, :] for h in halves], axis=0)
        turned_rot = jnp.concatenate(
            [
                jnp.concatenate([h[HALF:PIECE, 0:HALF] for h in halves], axis=1),
                jnp.concatenate([h[HALF:PIECE, HALF:256] for h in halves], axis=1),
            ],
            axis=0,
        )
        keys = jnp.dot(rows_of, kup[...], preferred_element_type=F32) + lax.dot_general(
            turned_rot, spread[...], (((0,), (0,)), ((), ())), preferred_element_type=F32
        )
        values = lax.dot_general(
            vupt[...], rows_of, (((1,), (1,)), ((), ())), preferred_element_type=F32
        )
        return keys.astype(BF16), values.astype(BF16)

    def fold(halves, blocks):
        keys, values = project(halves)
        scores = jnp.dot(keys, qt[...], preferred_element_type=F32) * factor
        if blocks is None:
            seen = lax.broadcasted_iota(jnp.int32, scores.shape, 0) <= (
                lax.broadcasted_iota(jnp.int32, scores.shape, 1) & 255
            )
            scores = jnp.where(seen, scores, NEGATIVE)
        else:
            scores = jnp.concatenate(
                [
                    scores[i * HALF : (i + 1) * HALF] + jnp.where(o <= sp, 0.0, NEGATIVE).astype(F32)
                    for i, o in enumerate(blocks)
                ],
                axis=0,
            )
        old = peak[...]
        new = jnp.maximum(old, jnp.max(scores, axis=0, keepdims=True))
        shrink = jnp.exp2(old - new)
        wt = jnp.exp2(scores - new)
        peak[...] = new
        total[...] = total[...] * shrink + jnp.sum(wt, axis=0, keepdims=True)
        wt = wt.astype(BF16)
        accum[0:128, :] = accum[0:128, :] * shrink[:, 0:256] + jnp.dot(
            values[0:128], wt[:, 0:256], preferred_element_type=F32
        )
        accum[128:192, :] = accum[128:192, :] * shrink[:, 256:512] + jnp.dot(
            values[128:192], wt[:, 256:512], preferred_element_type=F32
        )

    def begin(halves, slot):
        keys, vals = project(halves)
        raw = jnp.dot(keys, qt[...], preferred_element_type=F32)
        score[slot] = raw
        value[slot] = vals
        for i in range(4):
            most[slot, i : i + 1, :] = jnp.max(raw[i * HALF : (i + 1) * HALF], axis=0, keepdims=True)

    def finish(blocks, there, slot):
        hidden = [jnp.where((o <= sp) & there, 0.0, NEGATIVE).astype(F32) for o in blocks]
        old = peak[...]
        new = old
        for i in range(4):
            new = jnp.maximum(new, most[slot, i : i + 1, :] * factor + hidden[i])
        shrink = jnp.exp2(old - new)
        peak[...] = new
        parts = [
            jnp.exp2(score[slot, i * HALF : (i + 1) * HALF, :] * factor - (new - hidden[i])) for i in range(4)
        ]
        total[...] = total[...] * shrink + jnp.sum(
            (parts[0] + parts[1]) + (parts[2] + parts[3]), axis=0, keepdims=True
        )
        wt = jnp.concatenate([p.astype(BF16) for p in parts], axis=0)
        accum[0:128, :] = accum[0:128, :] * shrink[:, 0:256] + jnp.dot(
            value[slot, 0:128, :], wt[:, 0:256], preferred_element_type=F32
        )
        accum[128:192, :] = accum[128:192, :] * shrink[:, 256:512] + jnp.dot(
            value[slot, 128:192, :], wt[:, 256:512], preferred_element_type=F32
        )

    peak[...] = jnp.full_like(peak, NEGATIVE)
    total[...] = jnp.zeros_like(total)
    accum[...] = jnp.zeros_like(accum)
    fold([pieces.at[0], pieces.at[1]], None)

    def given(n, count):
        ref = two if count == 2 else lat.at[0, 0]
        remote(ref, ref, p_send.at[0], p_recv.at[n], partner).wait_recv()

    def blocks_of(n):
        kp, km, d = ring_step(n)
        return (
            at(a + rel(kp), b - d), at(a + rel(km), b + d), turned(b + rel(kp), a - d), turned(b + rel(km), a + d)
        )

    def halves_of(o):
        return [lat.at[core, o[0]], lat.at[core, o[1]], lat.at[other, o[2]], lat.at[other, o[3]]]

    def least(o):
        return jnp.minimum(jnp.minimum(o[0], o[1]), jnp.minimum(o[2], o[3]))

    def near_blocks(n):
        return at(a + rel(n), b), turned(b + rel(n), a)

    latents.spread(jnp.int32(0), pieces.at[core])

    def near_pair(n, slot):
        given(n, 1)
        given(n + 1, 1)
        one, two_ = near_blocks(n), near_blocks(n + 1)
        o = (one[0], two_[0], one[1], two_[1])
        begin(halves_of(o), slot)
        return o

    one_, two__, three, four, five, six, seven = (jnp.int32(i) for i in range(1, 8))
    latent_near(one_)
    latent_near(two__)
    latent_near(three)
    latent_near(four)
    latents.spread(one_)
    latents.spread(two__)
    wown[...] = jnp.zeros_like(wown)
    wown[:, 0:352] = gate_w[...]
    wown[:, 384:736] = up_w[...]
    wown[:, 768:1120] = down_w[...]
    score[...] = jnp.zeros_like(score)
    value[...] = jnp.zeros_like(value)
    most[...] = jnp.zeros_like(most)
    finish(near_pair(one_, 0), sp >= 0, 0)
    latents.spread(three)
    latents.spread(four)
    latent_far(jnp.int32(8))
    finish(near_pair(three, 0), sp >= 0, 0)
    latent_near(five)
    latent_near(six)
    latent_near(seven)
    latents.spread(five)
    latents.spread(six)
    latents.spread(seven)
    latent_far(jnp.int32(9))
    latent_far(jnp.int32(10))
    last_near = near_pair(five, 1)
    given(jnp.int32(7), 1)
    seventh = near_blocks(jnp.int32(7))

    @pl.when(jnp.minimum(seventh[0], seventh[1]) <= sp)
    def _():
        fold([lat.at[core, seventh[0]], lat.at[other, seventh[1]]], seventh)

    @pl.loop(0, 14)
    def _(m):
        n = 8 + 2 * m

        @pl.when(n + 3 < 36)
        def _():
            latent_far(n + 3)

        @pl.when(n + 4 < 36)
        def _():
            latent_far(n + 4)

        @pl.when(m == 1)
        def _():
            weights.start()

        @pl.when((m == 4) | (m == 6) | (m == 8))
        def _():
            weights.near(m - 3)
            weights.near(m - 2)

        @pl.when(m == 10)
        def _():
            weights.near(m - 3)
            weights.spread(jnp.int32(0), wown)

            @pl.loop(1, 8)
            def _(k):
                weights.spread(k)

        @pl.when(m == 12)
        def _():
            weights.far(jnp.int32(8))

        @pl.when(m == 13)
        def _():
            weights.far(jnp.int32(9))
            weights.far(jnp.int32(10))

        @pl.when(m == 5)
        def _():
            share_rows()

        @pl.when(m == 9)
        def _():
            share_near()

        now, after = blocks_of(n), blocks_of(n + 1)
        past = blocks_of(n - 1)
        before = [jnp.where(m == 0, o, p) for o, p in zip(last_near, past)]
        given(n, 2)
        given(n + 1, 2)

        @pl.when(jnp.minimum(jnp.minimum(least(before), least(now)), least(after)) <= sp)
        def _():
            begin(halves_of(now), 0)
            finish(before, m >= 0, 1)
            begin(halves_of(after), 1)
            finish(now, m >= 0, 0)

    finish(blocks_of(jnp.int32(35)), sp >= 0, 1)

    result = accum[...]
    att[tp, 0:128, :] = (result[0:128] / total[:, 0:256]).astype(BF16)
    att[tp, 128:192, :] = (result[128:192] / total[:, 256:512]).astype(BF16)

    share_far()

    def att_copy(t, half, i, dev):
        ref = att.at[t] if half is None else att.at[t, half]
        return remote(ref, ref, a_send.at[i], a_recv.at[i], dev)

    for half, i, dev in ((top, 0, x_up), (low, 2, x_dn), (low, 1, x_up), (top, 3, x_dn), (None, 6, partner)):
        att_copy(tp, half, i, dev).start()

    @pl.loop(11, 17)
    def _(n):
        weights.far(n)

    t_up, t_dn, t_far = across(3), across(1), across(2)
    att_copy(t_up, top, 0, partner).wait_recv()
    att_copy(t_up, top, 4, x_up).start()
    att_copy(t_dn, low, 2, partner).wait_recv()
    att_copy(t_dn, low, 5, x_dn).start()
    weights.far(jnp.int32(17))
    weights.far(jnp.int32(18))
    att_copy(t_up, low, 1, partner).wait_recv()
    att_copy(t_up, None, 8, partner).start()
    att_copy(t_dn, top, 3, partner).wait_recv()
    att_copy(t_dn, None, 7, partner).start()

    @pl.loop(19, 21)
    def _(n):
        weights.far(n)

    att_copy(t_far, top, 4, partner).wait_recv()
    att_copy(t_far, top, 9, partner).start()
    att_copy(t_far, low, 5, partner).wait_recv()
    att_copy(t_far, low, 10, partner).start()
    weights.far(jnp.int32(21))
    weights.far(jnp.int32(22))

    for half, i in ((None, 6), (None, 7), (None, 8), (top, 9), (low, 10)):
        att_copy(tp, half, i, partner).wait_recv()

    for i in (0, 1, 2, 3):
        t = 2 * rem(xx + i, 4) + other
        remote(rows.at[t], rows.at[t], r_send.at[0], r_recv.at[t], partner).wait_recv()
        if i == 2:
            for j, rest in ((10, top), (11, low)):
                remote(wout.at[t, rest], wout.at[t, rest], o_send.at[0], o_recv.at[j], partner).wait_recv()
        else:
            remote(wout.at[t], wout.at[t], o_send.at[0], o_recv.at[t], partner).wait_recv()

    @pl.loop(0, 8)
    def _(t):
        att_t[t] = att[t].T

    @pl.loop(0, 4)
    def _(j):
        cols = pl.ds(pl.multiple_of(j * 512, 512), 512)
        acc = jnp.dot(att_t[0], wout[0, :, cols], preferred_element_type=F32)
        for t in range(1, 8):
            acc = acc + jnp.dot(att_t[t], wout[t, :, cols], preferred_element_type=F32)
        hs[:, cols] = acc
        weights.far(23 + 2 * j)
        weights.far(24 + 2 * j)

    for i in range(7):
        remote(rows.at[tp], rows.at[tp], r_send.at[i], r_recv.at[tp], partner).wait_send()

    @pl.loop(0, 8)
    def _(t):
        chunk = pl.ds(pl.multiple_of(t * 32, 32), 32)
        value = hs[chunk, :]
        scale = lax.rsqrt(jnp.mean(value * value, axis=-1, keepdims=True) + EPS)
        mixed = (rows[t].astype(F32) + value * scale * again[...]).astype(BF16)
        rows[t] = mixed
        value = mixed.astype(F32)
        scale = lax.rsqrt(jnp.mean(value * value, axis=-1, keepdims=True) + EPS)
        norm[chunk, :] = (value * scale * mgain[...]).astype(BF16)

        @pl.when(t < 5)
        def _():
            weights.far(31 + t)


    wts[sp] = wown[...]
    both = jnp.dot(norm[...], wts[:, :, 0:768].reshape(2048, 768), preferred_element_type=F32)
    gate, up = both[:, 0:384], both[:, 384:768]
    hid[...] = (gate / (1.0 + jnp.exp(-gate)) * up).astype(BF16)

    @pl.loop(0, 2)
    def _(j):
        down = wts[pl.ds(j * 32, 32), :, 768:1152].reshape(1024, 384)
        block = lax.dot_general(hid[...], down, (((1,), (1,)), ((), ())), preferred_element_type=F32)
        part[:, :, pl.ds(pl.multiple_of(j * 1024, 1024), 1024)] = block.astype(BF16).reshape(8, 32, 1024)

    for i in (2, 1, 3, 0):
        x_to = rem(xx + i, 4)
        remote(part.at[2 * x_to + other], pbuf.at[x_to], s_send.at[i], s_recv.at[i], partner).start()
    def chip_sum(i):
        x_to = rem(xx + i, 4)
        remote(pbuf.at[x_to], pbuf.at[x_to], s_send.at[i], s_recv.at[i], partner).wait_recv()
        return part[2 * x_to + core].astype(F32) + pbuf[x_to].astype(F32)

    upper, under = pl.ds(0, 16), pl.ds(16, 16)

    def along(src, dst, i, dev):
        return remote(src, dst, s_send.at[i], s_recv.at[i], dev)

    far_sum = chip_sum(2)
    sbuf[1] = far_sum.astype(BF16)
    up_sum = chip_sum(1)
    sbuf[0] = up_sum.astype(BF16)
    along(sbuf.at[1, upper], rbuf.at[1, upper], 4, x_up).start()
    along(sbuf.at[1, under], rbuf.at[1, under], 5, x_dn).start()
    dn_sum = chip_sum(3)
    sbuf[2] = dn_sum.astype(BF16)
    along(sbuf.at[0, under], rbuf.at[0, under], 6, x_up).start()
    summed = chip_sum(0)
    along(sbuf.at[2, upper], rbuf.at[2, upper], 7, x_dn).start()

    @pl.loop(0, 8)
    def _(n):
        for sems in (plus, minus):
            weights.free(sems.at[n])
        given_free(n, 2)

        @pl.when(n != 6)
        def _():
            weights.free(first.at[n])

    for i in range(11):
        half = (top, low, low, top, top, low, None, None, None, top, low)[i]
        att_copy(tp, half, i, partner).wait_send()
    for i in (0, 1, 2, 5, 6):
        remote(wout.at[tp], wout.at[tp], o_send.at[i], o_recv.at[tp], partner).wait_send()
    for i in (3, 4, 7, 8):
        remote(wout.at[tp, top], wout.at[tp, top], o_send.at[i], o_recv.at[tp], partner).wait_send()

    along(rbuf.at[1, upper], rbuf.at[1, upper], 4, partner).wait_recv()
    cbuf[0] = (sums_of(part, pbuf, rem(xx + 1, 4), core, 0) + rbuf[1, 0:16].astype(F32)).astype(BF16)
    along(rbuf.at[1, under], rbuf.at[1, under], 5, partner).wait_recv()
    cbuf[1] = (sums_of(part, pbuf, rem(xx + 3, 4), core, 16) + rbuf[1, 16:32].astype(F32)).astype(BF16)
    along(cbuf.at[0], rbuf.at[0, upper], 8, x_up).start()
    along(cbuf.at[1], rbuf.at[2, under], 9, x_dn).start()
    along(rbuf.at[0, under], rbuf.at[0, under], 6, partner).wait_recv()
    along(rbuf.at[2, upper], rbuf.at[2, upper], 7, partner).wait_recv()
    along(rbuf.at[0, upper], rbuf.at[0, upper], 8, partner).wait_recv()
    along(rbuf.at[2, under], rbuf.at[2, under], 9, partner).wait_recv()
    summed = summed + (rbuf[0].astype(F32) + rbuf[2].astype(F32))
    out[...] = (rows[tp].astype(F32) + 0.5 * summed).astype(BF16)

    for i in range(4):
        remote(rbuf.at[0], rbuf.at[0], s_send.at[i], s_recv.at[i], partner).wait_send()
    for i in range(4, 10):
        along(rbuf.at[0, upper], rbuf.at[0, upper], i, partner).wait_send()


def sums_of(part, pbuf, x_to, core, start):
    rows = slice(start, start + 16)
    return part[2 * x_to + core, rows].astype(F32) + pbuf[x_to, rows].astype(F32)


def shards(
    residual_in, query_lean, query_broad, latent, rope_key, latent_gain, key_up_lean, key_up_broad, value_up_lean,
    value_up_broad, out_lean, out_broad, attn_gain, mlp_gain, gate_weight, up_weight, down_weight,
):
    tokens = latent.shape[0]
    positions = lax.axis_index("sp") * tokens + jnp.arange(tokens, dtype=jnp.int32)
    freqs = THETA ** (-2.0 * jnp.arange(16, dtype=F32) / 32)
    angle = freqs[:, None] * positions.astype(F32)[None, :]
    vmem = pl.BlockSpec(memory_space=pltpu.VMEM)
    hbm = pl.BlockSpec(memory_space=pl.ANY)
    sems = pltpu.SemaphoreType.DMA
    loaded = [
        ((256, 256), BF16), ((1, 256), F32), ((32, 256), BF16), ((16, 256), F32), ((16, 256), F32), ((160, 256), BF16),
        ((96, 256), BF16), ((256, 128), BF16), ((64, 256), BF16), ((256, 128), BF16), ((64, 256), BF16),
        ((1, 2048), F32), ((1, 2048), F32), ((32, 352), BF16), ((32, 352), BF16), ((32, 352), BF16),
    ]
    scratch = [pltpu.VMEM(shape, dtype) for shape, dtype in loaded] + [
        pltpu.VMEM((2, PIECE, 256), BF16),
        pltpu.VMEM((2, 512, 512), F32),
        pltpu.VMEM((2, 192, 512), BF16),
        pltpu.VMEM((2, 8, 512), F32),
        pltpu.VMEM((2, 64, PIECE, 256), BF16),
        pltpu.VMEM((64, 32, 1152), BF16),
        pltpu.VMEM((8, 192, 2048), BF16),
        pltpu.VMEM((8, 32, 2048), BF16),
        pltpu.VMEM((8, 192, 256), BF16),
        pltpu.VMEM((256, 512), BF16),
        pltpu.VMEM((256, 256), BF16),
        pltpu.VMEM((192, 256), BF16),
        pltpu.VMEM((32, 256), BF16),
        pltpu.VMEM((1, 512), F32),
        pltpu.VMEM((1, 512), F32),
        pltpu.VMEM((192, 256), F32),
        pltpu.VMEM((8, 256, 192), BF16),
        pltpu.VMEM((256, 2048), F32),
        pltpu.VMEM((256, 2048), BF16),
        pltpu.VMEM((256, 384), BF16),
        pltpu.VMEM((8, 32, 2048), BF16),
        pltpu.VMEM((4, 32, 2048), BF16),
        pltpu.VMEM((3, 32, 2048), BF16),
        pltpu.VMEM((3, 32, 2048), BF16),
        pltpu.VMEM((2, 16, 2048), BF16),
        pltpu.VMEM((32, 1152), BF16),
        sems((36,)), sems((36,)), sems((36,)), sems((8,)), sems((8,)), sems((8,)), sems((8,)),
        sems((3,)), sems((9,)), sems((12,)), sems((7,)), sems((8,)), sems((11,)), sems((11,)), sems((10,)), sems((10,)),
        sems((16,)),
    ]
    return pl.pallas_call(
        kernel,
        out_shape=jax.ShapeDtypeStruct((32, 2048), BF16),
        in_specs=[hbm] * 19,
        out_specs=vmem,
        scratch_shapes=scratch,
        compiler_params=pltpu.CompilerParams(
            collective_id=0, has_side_effects=True, vmem_limit_bytes=44 * 1024 * 1024
        ),
    )(
        *[pltpu.with_memory_space_constraint(v, pltpu.HBM) for v in (latent, latent_gain[None], rope_key.T)],
        jnp.cos(angle),
        jnp.sin(angle),
        *[
            pltpu.with_memory_space_constraint(v, pltpu.HBM)
            for v in (
                query_broad[:, 0].T, query_lean[:, 0].T, key_up_broad[:, 0], key_up_lean[:, 0].T, value_up_broad[:, 0],
                value_up_lean[:, 0].T, attn_gain[None], mlp_gain[None], gate_weight, up_weight, down_weight.T,
                out_broad[0], out_lean[0], residual_in,
            )
        ],
    )


def solution(mesh):
    in_specs = (
        P(("sp", "tp"), None), P("sp", "tp", None), P("sp", "tp", None), P("sp", None), P("sp", None), P(),
        P(None, "tp", None), P(None, "tp", None), P(None, "tp", None), P(None, "tp", None),
        P("tp", None, None), P("tp", None, None), P(), P(), P("sp", "tp"), P("sp", "tp"), P("tp", "sp"),
    )
    return jax.shard_map(
        shards, mesh=mesh, in_specs=in_specs, out_specs=P(("sp", "tp"), None), check_vma=False
    )
```
